512 devices in a mesh: sp: 32 (over z, x), tp: 16 (over y, core).
Axes of the slice: x: 4, y: 8, z: 8, core: 2. Of those that a mesh axis runs over, the one named last changes fastest.
Arguments:
- conv_value: bfloat16 [8192, 1024], P('sp', 'tp'), may hold values from -15 to 15
- conv_gate: bfloat16 [8192, 1024], P('sp', 'tp'), may hold values from -8 to 8
- conv_taps: bfloat16 [31, 1024], P(None, 'tp'), may hold values from -1 to 1
- conv_gain: float32 [1024], P('tp'), may hold values from 0.1 to 1.9
- out_weight: bfloat16 [1024, 2048], P('tp'), may hold values from -0.1875 to 0.1875
- residual: bfloat16 [8192, 2048], P('sp'), may hold values from -6 to 6
- route_ids: int32 [8192, 2], P('sp'), may hold values from 0 to 31, all different within a row; in each aligned block of 256 rows (0 to 255, 256 to 511, ...) at most 32 rows name the same one
- route_weight: float32 [8192, 2], P('sp'), may hold values from 0.3 to 1.5
- expert_gate: bfloat16 [32, 2048, 4096], P('sp', None, 'tp'), may hold values from -0.125 to 0.125
- expert_up: bfloat16 [32, 2048, 4096], P('sp', None, 'tp'), may hold values from -0.125 to 0.125
- expert_down: bfloat16 [32, 4096, 2048], P('sp', 'tp'), may hold values from -0.09375 to 0.09375
Outputs:
- layer_out: bfloat16 [8192, 2048], P('sp', 'tp')
The draws below stay inside these ranges and needn't reach their ends.
Inputs may be any that keep to these rules, and one draw needn't show every extreme that they name: `route_ids`: in each aligned block of 256 rows no expert is named by more than 32 rows; some expert is named by exactly 32 rows in some blocks.
All inputs are finite; a program needn't handle non-finite values.
Results may differ from the reference program's by a relative error of at most 0.017.
Values may be sent and summed in bfloat16 or wider, within the bound.
No kernel may reach another device: no remote copies, remote signals or barrier semaphores. Data moves between devices by JAX's collectives and lax.ppermute only.
A program may use at most 64 MiB of HBM per device.

```python
import math
from functools import partial
import jax
import jax.numpy as jnp
import numpy as np
from jax import lax

D = 2048
CH = 1024
KW = 31
EXPERT_FF = 4096
TOP_K = 2
TOK_DEV = 256
TOKENS = 8192
EXPERTS = 32
CAP = 32
N_SP = 32
N_TP = 16


def draw_conv_value(key, part):
    spread = jnp.exp(jnp.log(6.0) * jnp.arange(CH, dtype=jnp.float32) / CH)
    sample = jnp.clip(jax.random.normal(key, (TOKENS, CH), jnp.float32), -5.0, 5.0)
    return (0.5 * sample * spread[None, :]).astype(jnp.bfloat16)


def levels(stream_key, dims, cuts, low, largest):
    def one(dim, blocks):
        steps = jax.random.uniform(jax.random.fold_in(jax.random.fold_in(stream_key, 6), dim), (blocks,), jnp.float32, low / len(cuts), largest / len(cuts))
        return jnp.repeat(jnp.exp(steps), dims[dim] // blocks).reshape((-1,) + (1,) * (len(dims) - dim - 1))

    level = one(*cuts[0])
    for cut in cuts[1:]:
        level = level * one(*cut)
    return level


def routed_block(own_key, own, number, rows, amount, top, bound, lean):
    order = jax.random.permutation(own_key, amount)
    crowded, usual = load_shares(amount, rows * top, bound, lean, True), load_shares(amount, rows * top, bound, lean, False)
    places = jnp.arange(amount)

    def named(lengths, turn):
        used = int((lengths > 0).sum())
        fixed = max(1, used // 4)
        moved = fixed + (places - fixed + turn * (used - fixed)) % max(1, amount - fixed)
        return jnp.zeros((amount,), jnp.int32).at[order[jnp.where(places < fixed, places, moved)]].set(jnp.asarray(lengths, jnp.int32))

    lengths = jnp.where(number % 4 == 0, named(crowded, number // 4), named(usual, number - number // 4 - 1))
    mixed = jax.random.permutation(jax.random.fold_in(own, 3), amount)
    source_of, receiver = mixed[0:amount // 2 * 2:2], mixed[1:amount // 2 * 2:2]
    room = jnp.minimum(lengths[source_of] - 1, bound - lengths[receiver]) // 2
    room = jnp.where((source_of == order[0]) | (receiver == order[0]) | (lengths[receiver] == 0), 0, jnp.maximum(room, 0))
    moved = jax.random.randint(jax.random.fold_in(own, 4), (amount // 2,), 0, 1 << 20) % (room + 1)
    lengths = lengths.at[source_of].add(-moved).at[receiver].add(moved)
    members = jnp.searchsorted(jnp.cumsum(lengths), jnp.arange(rows * top), side="right").astype(jnp.int32)
    table = members.reshape(top, rows).T
    table = table[jax.random.permutation(jax.random.fold_in(own, 1), rows)]
    turn = jax.random.randint(jax.random.fold_in(own, 2), (rows, 1), 0, top)
    return jnp.take_along_axis(table, (jnp.arange(top)[None, :] + turn) % top, axis=1)


def load_shares(count, total, bound, lean, full):
    portions = [(1 << 20) // math.isqrt(standing ** lean) + 1 for standing in range(1, count + 1)]
    largest = bound if full else min(bound, max(-(-total // count), total * portions[0] // sum(portions)))
    least = 1 if total - largest >= count - 1 else 0
    given, rest = [largest] + [least] * (count - 1), total - largest - least * (count - 1)
    while rest > 0:
        free = [i for i in range(1, count) if given[i] < largest] or [i for i in range(1, count) if given[i] < bound]
        whole, budget = sum([portions[i] for i in free]), rest
        for i in free:
            addition = min(bound - given[i], max(1, budget * portions[i] // whole), rest)
            given[i] = given[i] + addition
            rest = rest - addition
    return np.array(given)


def gaussian(stream_key, shape, width, most, split=(), held_as=jnp.bfloat16):
    array = width * jax.random.normal(stream_key, shape, jnp.float32)
    if split:
        array = array * levels(stream_key, shape, split, -0.22, 0.18)
    return jnp.clip(array, -most, most).astype(held_as)


def setup_inputs(seed: int = 0) -> dict:
    key_of = jax.random.split(jax.random.key(seed), 12)
    conv_value = draw_conv_value(jax.random.fold_in(key_of[11], 71), 0)
    conv_gate = gaussian(key_of[1], (TOKENS, CH), 1.5, 8.0, ((0, 32), (1, 16)))
    conv_taps = gaussian(key_of[2], (KW, CH), KW ** -0.5, 1.0, ((1, 16),))
    conv_gain = jnp.clip(1.0 + 0.18 * jax.random.normal(key_of[3], (CH,), jnp.float32), 0.1, 1.9)
    out_weight = gaussian(key_of[4], (CH, D), CH ** -0.5, 0.1875, ((0, 16),))
    residual = gaussian(key_of[5], (TOKENS, D), 1.0, 6.0, ((0, 32),))
    route_ids_keys = jax.random.split(jax.random.fold_in(key_of[6], 1), TOKENS // TOK_DEV)
    route_ids_turns = jax.random.permutation(jax.random.fold_in(key_of[6], 3), TOKENS // TOK_DEV)
    route_ids = jax.vmap(lambda own, number: routed_block(jax.random.fold_in(key_of[6], 2), own, number, TOK_DEV, EXPERTS, TOP_K, CAP, 2))(route_ids_keys, route_ids_turns).reshape((TOKENS, TOP_K))
    route_weight = jnp.clip(jnp.exp(math.log(1.5) - 1.60943787 * jax.random.uniform(key_of[7], (TOKENS, TOP_K), jnp.float32) ** levels(key_of[7], (TOKENS, TOP_K), ((0, 32),), -0.2, 0.2)), 0.3, 1.5)
    expert_gate = gaussian(key_of[8], (EXPERTS, D, EXPERT_FF), D ** -0.5, 0.125, ((0, 32), (2, 16)))
    expert_up = gaussian(key_of[9], (EXPERTS, D, EXPERT_FF), D ** -0.5, 0.125, ((0, 32), (2, 16)))
    expert_down = gaussian(key_of[10], (EXPERTS, EXPERT_FF, D), EXPERT_FF ** -0.5, 0.09375, ((0, 32), (1, 16)))
    return {"conv_value": conv_value, "conv_gate": conv_gate, "conv_taps": conv_taps, "conv_gain": conv_gain, "out_weight": out_weight, "residual": residual, "route_ids": route_ids, "route_weight": route_weight, "expert_gate": expert_gate, "expert_up": expert_up, "expert_down": expert_down}


def slot_plan(block_ids, experts, capacity):
    assigned = block_ids.reshape(-1)
    pair_count = assigned.shape[0]
    onehot = (assigned[:, None] == jnp.arange(experts, dtype=jnp.int32)[None, :]).astype(jnp.int32)
    earlier = jnp.cumsum(onehot, axis=0) - onehot
    ranking = lax.optimization_barrier(jnp.sum(earlier * onehot, axis=1))
    target = assigned * capacity + ranking
    owners = jnp.arange(pair_count, dtype=jnp.int32) // block_ids.shape[1]
    matches = target[None, :] == jnp.arange(experts * capacity, dtype=jnp.int32)[:, None]
    holder = lax.optimization_barrier(jnp.sum(jnp.where(matches, owners[None, :] + 1, 0), axis=1)) - 1
    holder = jnp.where(holder < 0, block_ids.shape[0], holder)
    return (target.astype(jnp.int32), holder.astype(jnp.int32))

def reference(conv_value, conv_gate, conv_taps, conv_gain, out_weight, residual, route_ids, route_weight, expert_gate, expert_up, expert_down):
    gated = conv_value.astype(jnp.float32) * jax.nn.sigmoid(conv_gate.astype(jnp.float32))
    padded = jnp.pad(gated, ((KW - 1, 0), (0, 0)))
    filtered = jnp.zeros((TOKENS, CH), jnp.float32)
    for offset in range(KW):
        filtered = filtered + conv_taps[offset].astype(jnp.float32) * padded[offset:offset + TOKENS]
    average = lax.optimization_barrier(jnp.mean(filtered, axis=1, keepdims=True))
    variance = lax.optimization_barrier(jnp.mean(filtered * filtered, axis=1, keepdims=True)) - average * average
    normed = (filtered - average) * lax.rsqrt(variance + 1e-05) * conv_gain.astype(jnp.float32)
    activated = jax.nn.silu(normed).astype(jnp.bfloat16)
    group_width = CH // N_TP
    mixed = jnp.zeros((TOKENS, D), jnp.float32)
    for group in range(N_TP):
        product = jnp.dot(activated[:, group * group_width:(group + 1) * group_width], out_weight[group * group_width:(group + 1) * group_width], preferred_element_type=jnp.float32)
        mixed = mixed + lax.optimization_barrier(product.astype(jnp.bfloat16)).astype(jnp.float32)
    updated = residual.astype(jnp.float32) + mixed
    normal_rows = (updated * lax.rsqrt(lax.optimization_barrier(jnp.mean(updated * updated, axis=1, keepdims=True)) + 1e-06)).astype(jnp.bfloat16)
    row_blocks = normal_rows.reshape(N_SP, TOK_DEV, D)
    id_blocks = route_ids.reshape(N_SP, TOK_DEV, TOP_K)
    targets, holders = jax.vmap(partial(slot_plan, experts=EXPERTS, capacity=CAP))(id_blocks)
    padded_rows = jnp.concatenate([row_blocks, jnp.zeros((N_SP, 1, D), jnp.bfloat16)], axis=1)
    expert_in = jnp.take_along_axis(padded_rows, holders[:, :, None], axis=1)
    expert_in = jnp.moveaxis(expert_in.reshape(N_SP, EXPERTS, CAP, D), 1, 0).reshape(EXPERTS, N_SP * CAP, D)
    hidden_group = EXPERT_FF // N_TP

    def one_expert(packed):
        rows_in, w_gate, w_up, w_down = packed
        gate_act = jnp.dot(rows_in, w_gate, preferred_element_type=jnp.float32)
        up_act = jnp.dot(rows_in, w_up, preferred_element_type=jnp.float32)
        hidden = (jax.nn.silu(gate_act) * up_act).astype(jnp.bfloat16)
        split_hidden = hidden.reshape(-1, N_TP, hidden_group).astype(jnp.float32)
        split_down = w_down.reshape(N_TP, hidden_group, D).astype(jnp.float32)
        pieces = jnp.einsum('rgf,gfd->grd', split_hidden, split_down)
        pieces = lax.optimization_barrier(pieces.astype(jnp.bfloat16)).astype(jnp.float32)
        return lax.optimization_barrier(jnp.sum(pieces, axis=0)).astype(jnp.bfloat16)
    expert_out = lax.map(one_expert, (expert_in, expert_gate, expert_up, expert_down))
    returned = jnp.moveaxis(expert_out.reshape(EXPERTS, N_SP, CAP, D), 1, 0).reshape(N_SP, EXPERTS * CAP, D)
    picked = jnp.take_along_axis(returned, targets[:, :, None], axis=1).reshape(TOKENS, TOP_K, D)
    combined = lax.optimization_barrier(jnp.sum(picked.astype(jnp.float32) * route_weight[:, :, None], axis=1))
    return (updated + combined).astype(jnp.bfloat16)
```

```python
import jax
import jax.numpy as jnp
from jax import lax
from jax.experimental import pallas as pl
from jax.experimental.pallas import tpu as pltpu
from jax.sharding import Mesh
from jax.sharding import PartitionSpec as P

TP = ("y", "c")
VMEM = pl.BlockSpec(memory_space=pltpu.VMEM)
SMEM = pl.BlockSpec(memory_space=pltpu.SMEM)
F32 = jnp.float32
BF16 = jnp.bfloat16


def pieces(value):
    first = lax.reduce_precision(value, 8, 7)
    second = lax.reduce_precision(value - first, 8, 7)
    third = lax.reduce_precision(value - first - second, 8, 7)
    return first, second, third


def twin(value):
    return lax.ppermute(value, "c", [(0, 1), (1, 0)])


def across(contract_left, contract_right):
    return (((contract_left,), (contract_right,)), ((), ()))


def token_kernel(core_ref, rows_ref, own_ref, other_ref, res_ref, ids_ref, upd_ref, send_ref, rank_ref):
    core = core_ref[0]
    blocks, _, group, tokens = rows_ref.shape
    half = blocks * group
    width = res_ref.shape[1]
    own = rows_ref[:, core].reshape(half, tokens).astype(F32)
    other = rows_ref[:, 1 - core].reshape(half, tokens).astype(F32)
    channels = 2 * half
    total = jnp.sum(own, axis=0, keepdims=True) + jnp.sum(other, axis=0, keepdims=True)
    squares = jnp.sum(own * own, axis=0, keepdims=True) + jnp.sum(other * other, axis=0, keepdims=True)
    average = total / channels
    variance = squares / channels - average * average
    scale = lax.rsqrt(variance + 1e-05)
    mixed = jnp.zeros((tokens, width), F32)
    for values, weight_ref in ((own, own_ref), (other, other_ref)):
        weight = weight_ref[...].reshape(half, weight_ref.shape[2])
        parts = weight[:, width : width + 128].astype(F32)
        gain = parts[:, 0:1] + parts[:, 1:2] + parts[:, 2:3]
        normed = (values - average) * scale * gain
        activated = (normed / (1.0 + jnp.exp(-normed))).astype(BF16)
        mixed = mixed + lax.dot_general(
            activated, weight[:, :width], across(0, 0), preferred_element_type=F32
        )
    updated = res_ref[...].astype(F32) + mixed
    upd_ref[...] = updated
    experts, slots = send_ref.shape[:2]
    expert = lax.broadcasted_iota(jnp.int32, (experts, tokens), 0)
    named = (ids_ref[0:1, :] == expert) | (ids_ref[1:2, :] == expert)
    before = lax.broadcasted_iota(jnp.int32, (tokens, tokens), 0)
    after = lax.broadcasted_iota(jnp.int32, (tokens, tokens), 1)
    earlier = jnp.dot(
        named.astype(F32).astype(BF16),
        (before < after).astype(F32).astype(BF16),
        preferred_element_type=F32,
    )
    rank = jnp.where(named, earlier, -1.0)
    rank_ref[...] = rank
    slot = lax.broadcasted_iota(jnp.int32, (experts, slots, tokens), 1) + core * slots
    pick = (rank[:, None, :] == slot.astype(F32)).astype(F32).astype(BF16)
    sent = jnp.dot(
        pick.reshape(experts * slots, tokens), updated.astype(BF16), preferred_element_type=F32
    )
    send_ref[...] = sent.astype(BF16).reshape(experts, slots, width)


def expert_kernel(x_ref, g0_ref, g1_ref, u0_ref, u1_ref, d0_ref, d1_ref, out_ref):
    chunks, rows, width = x_ref.shape
    x = jnp.concatenate([x_ref[i] for i in range(chunks)], axis=1)
    squares = jnp.zeros((rows, 1), F32)
    for i in range(chunks):
        part = x_ref[i].astype(F32)
        squares = squares + jnp.sum(part * part, axis=1, keepdims=True)
    scale = lax.rsqrt(squares / (chunks * width) + 1e-06)
    result = jnp.zeros((rows, chunks * width), F32)
    for g_ref, u_ref, d_ref in ((g0_ref, u0_ref, d0_ref), (g1_ref, u1_ref, d1_ref)):
        gate = jnp.dot(x, g_ref[...], preferred_element_type=F32) * scale
        up = jnp.dot(x, u_ref[...], preferred_element_type=F32) * scale
        hidden = (gate / (1.0 + jnp.exp(-gate)) * up).astype(BF16)
        result = result + jnp.dot(hidden, d_ref[...], preferred_element_type=F32)
    for i in range(chunks):
        out_ref[i] = result[:, i * width : (i + 1) * width].astype(BF16)


def combine_kernel(core_ref, back_ref, rank_ref, ids_ref, w_ref, out_ref):
    core = core_ref[0]
    experts, slots, width = back_ref.shape
    tokens = rank_ref.shape[1]
    expert = lax.broadcasted_iota(jnp.int32, (experts, tokens), 0)
    weight = jnp.where(ids_ref[0:1, :] == expert, w_ref[0:1, :], 0.0) + jnp.where(
        ids_ref[1:2, :] == expert, w_ref[1:2, :], 0.0
    )
    slot = lax.broadcasted_iota(jnp.int32, (experts, slots, tokens), 1) + core * slots
    here = rank_ref[...][:, None, :] == slot.astype(F32)
    spread = jnp.where(here, weight[:, None, :], 0.0).reshape(experts * slots, tokens)
    back = back_ref[...].reshape(experts * slots, width)
    total = jnp.zeros((tokens, width), F32)
    for _ in range(3):
        piece = spread.astype(BF16)
        spread = spread - piece.astype(F32)
        total = total + lax.dot_general(piece, back, across(0, 0), preferred_element_type=F32)
    out_ref[...] = total


def local(
    conv_value,
    conv_gate,
    conv_taps,
    conv_gain,
    out_weight,
    residual,
    route_ids,
    route_weight,
    expert_gate,
    expert_up,
    expert_down,
):
    chips, experts = lax.axis_size("y"), lax.axis_size("sp")
    chip, core = lax.axis_index("y"), lax.axis_index("c")
    core_arg = core.astype(jnp.int32).reshape(1)
    taps_count, group = conv_taps.shape
    tokens = conv_value.shape[0]
    model = residual.shape[1]
    width = model // chips

    lanes = jnp.stack(pieces(conv_gain), axis=1).astype(BF16)
    lanes = jnp.broadcast_to(jnp.pad(lanes, ((0, 0), (0, 125)))[None], (chips, group, 128))
    columns = jnp.moveaxis(out_weight.reshape(group, chips, width), 1, 0)
    own_out = lax.all_to_all(jnp.concatenate([columns, lanes], axis=2), "y", 0, 0, tiled=True)
    other_out = twin(own_out)
    gates = (expert_gate[0], twin(expert_gate[0]))
    ups = (expert_up[0], twin(expert_up[0]))
    downs = (expert_down[0], twin(expert_down[0]))

    value, gate = conv_value.T.astype(F32), conv_gate.T.astype(F32)
    gated = value * jax.nn.sigmoid(gate)
    order = lax.axis_size("sp")
    head = lax.ppermute(
        gated[:, tokens - taps_count + 1 :], "sp", [(i, i + 1) for i in range(order - 1)]
    )
    gated = jnp.concatenate([head, gated], axis=1)
    taps = conv_taps.T.astype(F32)
    filtered = jnp.zeros((group, tokens), F32)
    for offset in range(taps_count):
        filtered = filtered + taps[:, offset : offset + 1] * gated[:, offset : offset + tokens]
    rows = lax.all_gather(filtered.astype(BF16), TP, axis=0, tiled=True)
    rows = rows.reshape(chips, 2, group, tokens)

    ids, weights = route_ids.T, route_weight.T
    res = lax.dynamic_slice_in_dim(residual, chip * width, width, 1)
    slots = 2 * tokens * route_ids.shape[1] // experts // 2
    updated, send, rank = pl.pallas_call(
        token_kernel,
        out_shape=(
            jax.ShapeDtypeStruct((tokens, width), F32),
            jax.ShapeDtypeStruct((experts, slots, width), BF16),
            jax.ShapeDtypeStruct((experts, tokens), F32),
        ),
        in_specs=[SMEM] + [VMEM] * 5,
        out_specs=(VMEM,) * 3,
        name="token",
    )(core_arg, rows, own_out, other_out, res, ids)

    arrived = lax.all_to_all(send, "sp", 0, 0, tiled=True).reshape(1, experts * slots, width)
    full = lax.all_gather(arrived, "y", axis=0, tiled=True)
    partial = pl.pallas_call(
        expert_kernel,
        out_shape=jax.ShapeDtypeStruct(full.shape, BF16),
        in_specs=[VMEM] * 7,
        out_specs=VMEM,
        name="expert",
    )(full, *gates, *ups, *downs)
    summed = lax.psum_scatter(partial, "y", scatter_dimension=0, tiled=True)
    back = lax.all_to_all(
        summed.reshape(experts, slots, width), "sp", 0, 0, tiled=True
    )
    part = pl.pallas_call(
        combine_kernel,
        out_shape=jax.ShapeDtypeStruct((tokens, width), F32),
        in_specs=[SMEM] + [VMEM] * 4,
        out_specs=VMEM,
        name="combine",
    )(core_arg, back, rank, ids, weights)
    mine = width // 2
    given = lax.dynamic_slice_in_dim(part, (1 - core) * mine, mine, 1)
    kept = lax.dynamic_slice_in_dim(part, core * mine, mine, 1)
    kept = kept + lax.dynamic_slice_in_dim(updated, core * mine, mine, 1)
    return (kept + twin(given)).astype(BF16)


def solution(mesh):
    grid = Mesh(mesh.devices.reshape(mesh.shape["sp"], 8, 2), ("sp", "y", "c"))
    placed = (
        P("sp", TP),
        P("sp", TP),
        P(None, TP),
        P(TP),
        P(TP, None),
        P("sp", None),
        P("sp", None),
        P("sp", None),
        P("sp", None, TP),
        P("sp", None, TP),
        P("sp", TP, None),
    )
    return jax.shard_map(local, mesh=grid, in_specs=placed, out_specs=P("sp", TP), check_vma=False)
```

```python
import jax
import jax.numpy as jnp
from jax import lax
from jax.experimental import pallas as pl
from jax.experimental.pallas import tpu as pltpu
from jax.sharding import Mesh
from jax.sharding import PartitionSpec as P

TP = ("y", "c")
VMEM = pl.BlockSpec(memory_space=pltpu.VMEM)
SMEM = pl.BlockSpec(memory_space=pltpu.SMEM)
HBM = pl.BlockSpec(memory_space=pltpu.HBM)
F32 = jnp.float32
BF16 = jnp.bfloat16


def twin(value):
    return lax.ppermute(value, "c", [(0, 1), (1, 0)])


def across(contract_left, contract_right):
    return (((contract_left,), (contract_right,)), ((), ()))


def room(mebibytes):
    return pltpu.CompilerParams(vmem_limit_bytes=mebibytes << 20)


def near(value):
    return pltpu.with_memory_space_constraint(value, pltpu.VMEM)


def far(value):
    return pltpu.with_memory_space_constraint(value, pltpu.HBM)


def gate_kernel(value_ref, gate_ref, out_ref, tail_ref):
    value, gate = value_ref[...].astype(F32), gate_ref[...].astype(F32)
    gated = value * (1.0 / (1.0 + jnp.exp(-gate)))
    out_ref[...] = gated
    tail_ref[...] = gated[:, gated.shape[1] - tail_ref.shape[1] :]


def pack_kernel(weight_ref, gain_ref, out_ref):
    chips, group, full = out_ref.shape
    width = full - 128
    rows = lax.broadcasted_iota(jnp.int32, (group, group), 0)
    lanes = lax.broadcasted_iota(jnp.int32, (group, group), 1)
    gain = jnp.sum(jnp.where(rows == lanes, gain_ref[...], 0.0), axis=1, keepdims=True)
    first = gain.astype(BF16).astype(F32)
    second = (gain - first).astype(BF16).astype(F32)
    third = gain - first - second
    lane = lax.broadcasted_iota(jnp.int32, (group, 128), 1)
    extra = jnp.where(lane == 0, first, jnp.where(lane == 1, second, jnp.where(lane == 2, third, 0.0)))
    extra = extra.astype(BF16)
    for i in range(chips):
        out_ref[i, :, :width] = weight_ref[:, i * width : (i + 1) * width]
        out_ref[i, :, width:] = extra


def filter_kernel(head_ref, gated_ref, taps_ref, out_ref):
    line = jnp.concatenate([head_ref[...], gated_ref[...]], axis=1)
    length, tokens = line.shape[1], out_ref.shape[1]
    count = taps_ref.shape[1]
    taps = taps_ref[...]
    total = jnp.zeros(out_ref.shape, F32)
    for i in range(count):
        begin = length - tokens - (count - 1) + i
        shifted = pltpu.roll(line, (length - begin) % length, 1)[:, :tokens]
        total = total + taps[:, i : i + 1] * shifted
    out_ref[...] = total.astype(out_ref.dtype)


def token_kernel(place_ref, rows_ref, own_ref, other_ref, ids_ref, all_ref, upd_ref, send_ref, rank_ref, res_ref, sem):
    chip, core = place_ref[0], place_ref[1]
    blocks, _, group, tokens = rows_ref.shape
    half = blocks * group
    width = res_ref.shape[1]
    columns = pl.ds(pl.multiple_of(chip * width, width), width)
    copy = pltpu.make_async_copy(all_ref.at[:, columns], res_ref, sem)
    copy.start()
    own = rows_ref[:, core].reshape(half, tokens).astype(F32)
    other = rows_ref[:, 1 - core].reshape(half, tokens).astype(F32)
    channels = 2 * half
    total = jnp.sum(own, axis=0, keepdims=True) + jnp.sum(other, axis=0, keepdims=True)
    squares = jnp.sum(own * own, axis=0, keepdims=True) + jnp.sum(other * other, axis=0, keepdims=True)
    average = total / channels
    variance = squares / channels - average * average
    scale = lax.rsqrt(variance + 1e-05)
    mixed = jnp.zeros((tokens, width), F32)
    for values, weight_ref in ((own, own_ref), (other, other_ref)):
        weight = weight_ref[...].reshape(half, weight_ref.shape[2])
        parts = weight[:, width : width + 128].astype(F32)
        gain = parts[:, 0:1] + parts[:, 1:2] + parts[:, 2:3]
        normed = (values - average) * scale * gain
        activated = (normed / (1.0 + jnp.exp(-normed))).astype(BF16)
        mixed = mixed + lax.dot_general(
            activated, weight[:, :width], across(0, 0), preferred_element_type=F32
        )
    copy.wait()
    updated = res_ref[...].astype(F32) + mixed
    mine = width // 2
    upd_ref[...] = jnp.where(core == 0, updated[:, :mine], updated[:, mine:])
    experts, slots = send_ref.shape[:2]
    expert = lax.broadcasted_iota(jnp.int32, (experts, tokens), 0)
    named = (ids_ref[0:1, :] == expert) | (ids_ref[1:2, :] == expert)
    before = lax.broadcasted_iota(jnp.int32, (tokens, tokens), 0)
    after = lax.broadcasted_iota(jnp.int32, (tokens, tokens), 1)
    earlier = jnp.dot(
        named.astype(F32).astype(BF16),
        (before < after).astype(F32).astype(BF16),
        preferred_element_type=F32,
    )
    rank = jnp.where(named, earlier, -1.0)
    rank_ref[...] = rank
    slot = lax.broadcasted_iota(jnp.int32, (experts, slots, tokens), 1) + core * slots
    pick = (rank[:, None, :] == slot.astype(F32)).astype(F32).astype(BF16)
    sent = jnp.dot(
        pick.reshape(experts * slots, tokens), updated.astype(BF16), preferred_element_type=F32
    )
    send_ref[...] = sent.astype(BF16).reshape(experts, slots, width)


def expert_kernel(x_hbm, *refs):
    weights_hbm, out_hbm = refs[:6], refs[6]
    x_ref, g0, g1, u0, u1, d0, d1, out_ref, in_sem, weight_sem, out_sem = refs[7:]
    chunks, rows, width = x_hbm.shape
    parts, part = x_ref.shape[0], x_ref.shape[2]
    ins = [
        pltpu.make_async_copy(x_hbm.at[:, pl.ds(k * part, part)], x_ref.at[k], in_sem.at[k])
        for k in range(parts)
    ]
    held = (g0, g1, u0, u1, d0, d1)
    moves = [pltpu.make_async_copy(weights_hbm[k], held[k], weight_sem.at[k]) for k in range(6)]
    ins[0].start()
    for k in (0, 2, 1, 3, 4, 5):
        moves[k].start()
    for k in range(1, parts):
        ins[k].start()
    outs = []
    for k in range(parts):
        ins[k].wait()
        x = jnp.concatenate([x_ref[k, i] for i in range(chunks)], axis=1)
        squares = jnp.zeros((part, 1), F32)
        for i in range(chunks):
            piece = x_ref[k, i].astype(F32)
            squares = squares + jnp.sum(piece * piece, axis=1, keepdims=True)
        scale = lax.rsqrt(squares / (chunks * width) + 1e-06)
        hidden = []
        for j in (0, 1):
            if k == 0:
                moves[j].wait()
            gate = jnp.dot(x, held[j][...], preferred_element_type=F32) * scale
            if k == 0:
                moves[2 + j].wait()
            up = jnp.dot(x, held[2 + j][...], preferred_element_type=F32) * scale
            hidden.append((gate / (1.0 + jnp.exp(-gate)) * up).astype(BF16))
        if k == 0:
            moves[4].wait()
            moves[5].wait()
        for i in range(chunks):
            columns = slice(i * width, (i + 1) * width)
            piece = jnp.dot(hidden[0], d0[:, columns], preferred_element_type=F32)
            piece = piece + jnp.dot(hidden[1], d1[:, columns], preferred_element_type=F32)
            out_ref[k, i] = piece.astype(BF16)
        out = pltpu.make_async_copy(out_ref.at[k], out_hbm.at[:, pl.ds(k * part, part)], out_sem.at[k])
        out.start()
        outs.append(out)
    for out in outs:
        out.wait()


def combine_kernel(place_ref, back_ref, rank_ref, ids_ref, w_ref, upd_ref, kept_ref, given_ref):
    core = place_ref[1]
    experts, slots, width = back_ref.shape
    tokens = rank_ref.shape[1]
    expert = lax.broadcasted_iota(jnp.int32, (experts, tokens), 0)
    weight = jnp.where(ids_ref[0:1, :] == expert, w_ref[0:1, :], 0.0) + jnp.where(
        ids_ref[1:2, :] == expert, w_ref[1:2, :], 0.0
    )
    slot = lax.broadcasted_iota(jnp.int32, (experts, slots, tokens), 1) + core * slots
    here = rank_ref[...][:, None, :] == slot.astype(F32)
    spread = jnp.where(here, weight[:, None, :], 0.0).reshape(experts * slots, tokens)
    back = back_ref[...].reshape(experts * slots, width)
    total = jnp.zeros((tokens, width), F32)
    for _ in range(3):
        piece = spread.astype(BF16)
        spread = spread - piece.astype(F32)
        total = total + lax.dot_general(piece, back, across(0, 0), preferred_element_type=F32)
    mine = width // 2
    low, high = total[:, :mine], total[:, mine:]
    kept_ref[...] = upd_ref[...] + jnp.where(core == 0, low, high)
    given_ref[...] = jnp.where(core == 0, high, low)


def local(
    conv_value,
    conv_gate,
    conv_taps,
    conv_gain,
    out_weight,
    residual,
    route_ids,
    route_weight,
    expert_gate,
    expert_up,
    expert_down,
):
    chips, experts = lax.axis_size("y"), lax.axis_size("sp")
    chip, core = lax.axis_index("y"), lax.axis_index("c")
    place = jnp.stack([chip, core]).astype(jnp.int32)
    taps_count, group = conv_taps.shape
    tokens = conv_value.shape[0]
    model = residual.shape[1]
    width = model // chips

    gated, tail = pl.pallas_call(
        gate_kernel,
        out_shape=(pltpu.VMEM((group, tokens), F32), pltpu.VMEM((group, 128), F32)),
        in_specs=[VMEM] * 2,
        out_specs=(VMEM,) * 2,
        compiler_params=room(4),
        name="gate",
    )(far(conv_value.T), far(conv_gate.T))
    tail, out_weight, conv_gain = lax.optimization_barrier((tail, out_weight, conv_gain))
    order = lax.axis_size("sp")
    head = lax.ppermute(tail, "sp", [(i, i + 1) for i in range(order - 1)])
    filtered = pl.pallas_call(
        filter_kernel,
        out_shape=pltpu.VMEM((group, tokens), BF16),
        in_specs=[VMEM] * 3,
        out_specs=VMEM,
        compiler_params=room(4),
        name="filter",
    )(near(head), near(gated), near(conv_taps.T.astype(F32)))
    rows = lax.all_gather(filtered, TP, axis=0, tiled=True)

    packed = pl.pallas_call(
        pack_kernel,
        out_shape=pltpu.VMEM((chips, group, width + 128), BF16),
        in_specs=[VMEM] * 2,
        out_specs=VMEM,
        compiler_params=room(4),
        name="pack",
    )(far(out_weight), far(conv_gain[None]))
    own_out = lax.all_to_all(packed, "y", 0, 0, tiled=True)
    rows, own_out = lax.optimization_barrier((rows, own_out))
    other_out = twin(own_out)
    rows = rows.reshape(chips, 2, group, tokens)
    gates = (expert_gate[0], twin(expert_gate[0]))
    ups = (expert_up[0], twin(expert_up[0]))
    downs = (expert_down[0], twin(expert_down[0]))

    ids, weights = route_ids.T, route_weight.T
    slots = 2 * tokens * route_ids.shape[1] // experts // 2
    mine = width // 2
    updated, send, rank = pl.pallas_call(
        token_kernel,
        out_shape=(
            pltpu.VMEM((tokens, mine), F32),
            pltpu.VMEM((experts, slots, width), BF16),
            pltpu.VMEM((experts, tokens), F32),
        ),
        in_specs=[SMEM] + [VMEM] * 4 + [HBM],
        out_specs=(VMEM,) * 3,
        scratch_shapes=[pltpu.VMEM((tokens, width), BF16), pltpu.SemaphoreType.DMA],
        compiler_params=room(12),
        name="token",
    )(place, near(rows), near(own_out), near(other_out), near(ids), far(residual))

    arrived = lax.all_to_all(send, "sp", 0, 0, tiled=True).reshape(1, experts * slots, width)
    full = lax.all_gather(arrived, "y", axis=0, tiled=True)
    parts, part = 2, full.shape[1] // 2
    partial = pl.pallas_call(
        expert_kernel,
        out_shape=pltpu.HBM(full.shape, BF16),
        in_specs=[HBM] * 7,
        out_specs=HBM,
        scratch_shapes=[
            pltpu.VMEM((parts, chips, part, width), BF16),
            *(pltpu.VMEM(w.shape, BF16) for w in (*gates, *ups, *downs)),
            pltpu.VMEM((parts, chips, part, width), BF16),
            pltpu.SemaphoreType.DMA((parts,)),
            pltpu.SemaphoreType.DMA((6,)),
            pltpu.SemaphoreType.DMA((parts,)),
        ],
        compiler_params=room(32),
        name="expert",
    )(far(full), *(far(w) for w in (*gates, *ups, *downs)))
    summed = lax.psum_scatter(partial, "y", scatter_dimension=0, tiled=True)
    back = lax.all_to_all(summed.reshape(experts, slots, width), "sp", 0, 0, tiled=True)
    kept, given = pl.pallas_call(
        combine_kernel,
        out_shape=(pltpu.VMEM((tokens, mine), F32), pltpu.VMEM((tokens, mine), F32)),
        in_specs=[SMEM] + [VMEM] * 5,
        out_specs=(VMEM,) * 2,
        compiler_params=room(8),
        name="combine",
    )(place, near(back), near(rank), near(ids), near(weights), near(updated))
    return (kept + twin(given)).astype(BF16)


def solution(mesh):
    grid = Mesh(mesh.devices.reshape(mesh.shape["sp"], 8, 2), ("sp", "y", "c"))
    placed = (
        P("sp", TP),
        P("sp", TP),
        P(None, TP),
        P(TP),
        P(TP, None),
        P("sp", None),
        P("sp", None),
        P("sp", None),
        P("sp", None, TP),
        P("sp", None, TP),
        P("sp", TP, None),
    )
    return jax.shard_map(local, mesh=grid, in_specs=placed, out_specs=P("sp", TP), check_vma=False)
```

```python
import jax
import jax.numpy as jnp
from jax import lax
from jax.experimental import pallas as pl
from jax.experimental.pallas import tpu as pltpu
from jax.sharding import Mesh
from jax.sharding import PartitionSpec as P

TP = ("y", "c")
VMEM = pl.BlockSpec(memory_space=pltpu.VMEM)
SMEM = pl.BlockSpec(memory_space=pltpu.SMEM)
HBM = pl.BlockSpec(memory_space=pltpu.HBM)
F32 = jnp.float32
BF16 = jnp.bfloat16


def twin(value):
    return lax.ppermute(value, "c", [(0, 1), (1, 0)])


def across(contract_left, contract_right):
    return (((contract_left,), (contract_right,)), ((), ()))


def room(mebibytes):
    return pltpu.CompilerParams(vmem_limit_bytes=mebibytes << 20)


def near(value):
    return pltpu.with_memory_space_constraint(value, pltpu.VMEM)


def far(value):
    return pltpu.with_memory_space_constraint(value, pltpu.HBM)


def gate_kernel(value_ref, gate_ref, out_ref, tail_ref):
    value, gate = value_ref[...].astype(F32), gate_ref[...].astype(F32)
    gated = value * (1.0 / (1.0 + jnp.exp(-gate)))
    out_ref[...] = gated
    tail_ref[...] = gated[:, gated.shape[1] - tail_ref.shape[1] :]


def pack_kernel(weight_ref, gain_ref, out_ref):
    chips, group, full = out_ref.shape
    width = full - 128
    rows = lax.broadcasted_iota(jnp.int32, (group, group), 0)
    lanes = lax.broadcasted_iota(jnp.int32, (group, group), 1)
    gain = jnp.sum(jnp.where(rows == lanes, gain_ref[...], 0.0), axis=1, keepdims=True)
    first = gain.astype(BF16).astype(F32)
    second = (gain - first).astype(BF16).astype(F32)
    third = gain - first - second
    lane = lax.broadcasted_iota(jnp.int32, (group, 128), 1)
    extra = jnp.where(lane == 0, first, jnp.where(lane == 1, second, jnp.where(lane == 2, third, 0.0)))
    extra = extra.astype(BF16)
    for i in range(chips):
        out_ref[i, :, :width] = weight_ref[:, i * width : (i + 1) * width]
        out_ref[i, :, width:] = extra


def filter_kernel(head_ref, gated_ref, taps_ref, out_ref):
    line = jnp.concatenate([head_ref[...], gated_ref[...]], axis=1)
    length, tokens = line.shape[1], out_ref.shape[1]
    count, group = taps_ref.shape
    same = lax.broadcasted_iota(jnp.int32, (group, group), 0) == lax.broadcasted_iota(
        jnp.int32, (group, group), 1
    )
    taps = lax.dot_general(
        same.astype(F32).astype(BF16), taps_ref[...], across(1, 1), preferred_element_type=F32
    )
    total = jnp.zeros(out_ref.shape, F32)
    for i in range(count):
        begin = length - tokens - (count - 1) + i
        shifted = pltpu.roll(line, (length - begin) % length, 1)[:, :tokens]
        total = total + taps[:, i : i + 1] * shifted
    out_ref[...] = total.astype(out_ref.dtype)


def token_kernel(place_ref, rows_ref, own_ref, other_ref, ids_ref, all_ref, upd_ref, send_ref, rank_ref, res_ref, sem):
    chip, core = place_ref[0], place_ref[1]
    blocks, _, group, tokens = rows_ref.shape
    half = blocks * group
    width = res_ref.shape[1]
    columns = pl.ds(pl.multiple_of(chip * width, width), width)
    copy = pltpu.make_async_copy(all_ref.at[:, columns], res_ref, sem)
    copy.start()
    own = rows_ref[:, core].reshape(half, tokens).astype(F32)
    other = rows_ref[:, 1 - core].reshape(half, tokens).astype(F32)
    channels = 2 * half
    total = jnp.sum(own, axis=0, keepdims=True) + jnp.sum(other, axis=0, keepdims=True)
    squares = jnp.sum(own * own, axis=0, keepdims=True) + jnp.sum(other * other, axis=0, keepdims=True)
    average = total / channels
    variance = squares / channels - average * average
    scale = lax.rsqrt(variance + 1e-05)
    mixed = jnp.zeros((tokens, width), F32)
    for values, weight_ref in ((own, own_ref), (other, other_ref)):
        weight = weight_ref[...].reshape(half, weight_ref.shape[2])
        parts = weight[:, width : width + 128].astype(F32)
        gain = parts[:, 0:1] + parts[:, 1:2] + parts[:, 2:3]
        normed = (values - average) * scale * gain
        activated = (normed / (1.0 + jnp.exp(-normed))).astype(BF16)
        mixed = mixed + lax.dot_general(
            activated, weight[:, :width], across(0, 0), preferred_element_type=F32
        )
    copy.wait()
    updated = res_ref[...].astype(F32) + mixed
    mine = width // 2
    upd_ref[...] = jnp.where(core == 0, updated[:, :mine], updated[:, mine:])
    experts, slots = send_ref.shape[:2]
    expert = lax.broadcasted_iota(jnp.int32, (experts, tokens), 0)
    named = (ids_ref[0:1, :] == expert) | (ids_ref[1:2, :] == expert)
    before = lax.broadcasted_iota(jnp.int32, (tokens, tokens), 0)
    after = lax.broadcasted_iota(jnp.int32, (tokens, tokens), 1)
    earlier = jnp.dot(
        named.astype(F32).astype(BF16),
        (before < after).astype(F32).astype(BF16),
        preferred_element_type=F32,
    )
    rank = jnp.where(named, earlier, -1.0)
    rank_ref[...] = rank
    slot = lax.broadcasted_iota(jnp.int32, (experts, slots, tokens), 1) + core * slots
    pick = (rank[:, None, :] == slot.astype(F32)).astype(F32).astype(BF16)
    sent = jnp.dot(
        pick.reshape(experts * slots, tokens), updated.astype(BF16), preferred_element_type=F32
    )
    send_ref[...] = sent.astype(BF16).reshape(experts, slots, width)


def expert_kernel(x_hbm, g0, g1, u0_hbm, u1_hbm, d0_hbm, d1_hbm, out_hbm, *refs):
    x_ref, up_ref, down_ref, out_ref, in_sem, up_sem, down_sem, out_sem = refs
    chunks, _, width = x_hbm.shape
    parts, part = x_ref.shape[0], x_ref.shape[2]
    half = d0_hbm.shape[0]
    ins = [
        pltpu.make_async_copy(x_hbm.at[:, pl.ds(k * part, part)], x_ref.at[k], in_sem.at[k])
        for k in range(parts)
    ]
    ups = [
        pltpu.make_async_copy(w, up_ref.at[k], up_sem.at[k]) for k, w in enumerate((u0_hbm, u1_hbm))
    ]
    downs = [
        pltpu.make_async_copy(w, down_ref.at[pl.ds(k * half, half)], down_sem.at[k])
        for k, w in enumerate((d0_hbm, d1_hbm))
    ]
    ins[0].start()
    ups[0].start()
    ups[1].start()
    outs = []
    for k in range(parts):
        ins[k].wait()
        if k == 0:
            downs[0].start()
            downs[1].start()
            for copy in ins[1:]:
                copy.start()
        x = jnp.concatenate([x_ref[k, i] for i in range(chunks)], axis=1)
        squares = jnp.zeros((part, 1), F32)
        for i in range(chunks):
            piece = x_ref[k, i].astype(F32)
            squares = squares + jnp.sum(piece * piece, axis=1, keepdims=True)
        scale = lax.rsqrt(squares / (chunks * width) + 1e-06)
        gates = [jnp.dot(x, g[...], preferred_element_type=F32) * scale for g in (g0, g1)]
        hidden = []
        for j, gate in enumerate(gates):
            if k == 0:
                ups[j].wait()
            up = jnp.dot(x, up_ref[j], preferred_element_type=F32) * scale
            hidden.append((gate / (1.0 + jnp.exp(-gate)) * up).astype(BF16))
        hidden = jnp.concatenate(hidden, axis=1)
        if k == 0:
            downs[0].wait()
            downs[1].wait()
        for i in range(chunks):
            columns = slice(i * width, (i + 1) * width)
            piece = jnp.dot(hidden, down_ref[:, columns], preferred_element_type=F32)
            out_ref[k, i] = piece.astype(BF16)
        out = pltpu.make_async_copy(out_ref.at[k], out_hbm.at[:, pl.ds(k * part, part)], out_sem.at[k])
        out.start()
        outs.append(out)
    for out in outs:
        out.wait()


def combine_kernel(place_ref, back_ref, rank_ref, ids_ref, w_ref, upd_ref, kept_ref, given_ref):
    core = place_ref[1]
    experts, slots, width = back_ref.shape
    tokens = rank_ref.shape[1]
    expert = lax.broadcasted_iota(jnp.int32, (experts, tokens), 0)
    weight = jnp.where(ids_ref[0:1, :] == expert, w_ref[0:1, :], 0.0) + jnp.where(
        ids_ref[1:2, :] == expert, w_ref[1:2, :], 0.0
    )
    slot = lax.broadcasted_iota(jnp.int32, (experts, slots, tokens), 1) + core * slots
    here = rank_ref[...][:, None, :] == slot.astype(F32)
    spread = jnp.where(here, weight[:, None, :], 0.0).reshape(experts * slots, tokens)
    back = back_ref[...].reshape(experts * slots, width)
    total = jnp.zeros((tokens, width), F32)
    for _ in range(3):
        piece = spread.astype(BF16)
        spread = spread - piece.astype(F32)
        total = total + lax.dot_general(piece, back, across(0, 0), preferred_element_type=F32)
    mine = width // 2
    low, high = total[:, :mine], total[:, mine:]
    kept_ref[...] = upd_ref[...] + jnp.where(core == 0, low, high)
    given_ref[...] = jnp.where(core == 0, high, low)


def local(
    conv_value,
    conv_gate,
    conv_taps,
    conv_gain,
    out_weight,
    residual,
    route_ids,
    route_weight,
    expert_gate,
    expert_up,
    expert_down,
):
    chips, experts = lax.axis_size("y"), lax.axis_size("sp")
    chip, core = lax.axis_index("y"), lax.axis_index("c")
    place = jnp.stack([chip, core]).astype(jnp.int32)
    _, group = conv_taps.shape
    tokens = conv_value.shape[0]
    model = residual.shape[1]
    width = model // chips

    gated, tail = pl.pallas_call(
        gate_kernel,
        out_shape=(pltpu.VMEM((group, tokens), F32), pltpu.VMEM((group, 128), F32)),
        in_specs=[VMEM] * 2,
        out_specs=(VMEM,) * 2,
        compiler_params=room(4),
        name="gate",
    )(far(conv_value.T), far(conv_gate.T))
    tail, out_weight, conv_gain = lax.optimization_barrier((tail, out_weight, conv_gain))
    order = lax.axis_size("sp")
    head = lax.ppermute(tail, "sp", [(i, i + 1) for i in range(order - 1)])
    filtered = pl.pallas_call(
        filter_kernel,
        out_shape=pltpu.VMEM((group, tokens), BF16),
        in_specs=[VMEM] * 3,
        out_specs=VMEM,
        compiler_params=room(4),
        name="filter",
    )(near(head), near(gated), far(conv_taps))
    rows = lax.all_gather(filtered, TP, axis=0, tiled=True)

    packed = pl.pallas_call(
        pack_kernel,
        out_shape=pltpu.VMEM((chips, group, width + 128), BF16),
        in_specs=[VMEM] * 2,
        out_specs=VMEM,
        compiler_params=room(4),
        name="pack",
    )(far(out_weight), far(conv_gain[None]))
    own_out = lax.all_to_all(packed, "y", 0, 0, tiled=True)
    rows, own_out = lax.optimization_barrier((rows, own_out))
    other_out = twin(own_out)
    rows = rows.reshape(chips, 2, group, tokens)
    gates = (expert_gate[0], twin(expert_gate[0]))
    ups = (expert_up[0], twin(expert_up[0]))
    downs = (expert_down[0], twin(expert_down[0]))

    ids, weights = route_ids.T, route_weight.T
    slots = 2 * tokens * route_ids.shape[1] // experts // 2
    mine = width // 2
    updated, send, rank = pl.pallas_call(
        token_kernel,
        out_shape=(
            pltpu.VMEM((tokens, mine), F32),
            pltpu.VMEM((experts, slots, width), BF16),
            pltpu.VMEM((experts, tokens), F32),
        ),
        in_specs=[SMEM] + [VMEM] * 4 + [HBM],
        out_specs=(VMEM,) * 3,
        scratch_shapes=[pltpu.VMEM((tokens, width), BF16), pltpu.SemaphoreType.DMA],
        compiler_params=room(12),
        name="token",
    )(place, near(rows), near(own_out), near(other_out), near(ids), far(residual))

    arrived = lax.all_to_all(send, "sp", 0, 0, tiled=True).reshape(1, experts * slots, width)
    full = lax.all_gather(arrived, "y", axis=0, tiled=True)
    parts, part = 2, full.shape[1] // 2
    partial = pl.pallas_call(
        expert_kernel,
        out_shape=pltpu.HBM(full.shape, BF16),
        in_specs=[HBM] + [VMEM] * 2 + [HBM] * 4,
        out_specs=HBM,
        scratch_shapes=[
            pltpu.VMEM((parts, chips, part, width), BF16),
            pltpu.VMEM((2, *ups[0].shape), BF16),
            pltpu.VMEM((2 * downs[0].shape[0], model), BF16),
            pltpu.VMEM((parts, chips, part, width), BF16),
            pltpu.SemaphoreType.DMA((parts,)),
            pltpu.SemaphoreType.DMA((2,)),
            pltpu.SemaphoreType.DMA((2,)),
            pltpu.SemaphoreType.DMA((parts,)),
        ],
        compiler_params=room(32),
        name="expert",
    )(far(full), *(near(w) for w in gates), *(far(w) for w in (*ups, *downs)))
    summed = lax.psum_scatter(partial, "y", scatter_dimension=0, tiled=True)
    back = lax.all_to_all(summed.reshape(experts, slots, width), "sp", 0, 0, tiled=True)
    kept, given = pl.pallas_call(
        combine_kernel,
        out_shape=(pltpu.VMEM((tokens, mine), F32), pltpu.VMEM((tokens, mine), F32)),
        in_specs=[SMEM] + [VMEM] * 5,
        out_specs=(VMEM,) * 2,
        compiler_params=room(8),
        name="combine",
    )(place, near(back), near(rank), near(ids), near(weights), near(updated))
    return (kept + twin(given)).astype(BF16)


def solution(mesh):
    grid = Mesh(mesh.devices.reshape(mesh.shape["sp"], 8, 2), ("sp", "y", "c"))
    placed = (
        P("sp", TP),
        P("sp", TP),
        P(None, TP),
        P(TP),
        P(TP, None),
        P("sp", None),
        P("sp", None),
        P("sp", None),
        P("sp", None, TP),
        P("sp", None, TP),
        P("sp", TP, None),
    )

    return jax.shard_map(local, mesh=grid, in_specs=placed, out_specs=P("sp", TP), check_vma=False)
```

```python
import jax
import jax.numpy as jnp
from jax import lax
from jax.experimental import pallas as pl
from jax.experimental.pallas import tpu as pltpu
from jax.sharding import Mesh
from jax.sharding import PartitionSpec as P

TP = ("y", "c")
VMEM = pl.BlockSpec(memory_space=pltpu.VMEM)
SMEM = pl.BlockSpec(memory_space=pltpu.SMEM)
HBM = pl.BlockSpec(memory_space=pltpu.HBM)
F32 = jnp.float32
BF16 = jnp.bfloat16


def twin(value):
    return lax.ppermute(value, "c", [(0, 1), (1, 0)])


def across(contract_left, contract_right):
    return (((contract_left,), (contract_right,)), ((), ()))


def room(mebibytes):
    return pltpu.CompilerParams(vmem_limit_bytes=mebibytes << 20)


def near(value):
    return pltpu.with_memory_space_constraint(value, pltpu.VMEM)


def far(value):
    return pltpu.with_memory_space_constraint(value, pltpu.HBM)


def gate_kernel(value_ref, gate_ref, out_ref, tail_ref):
    value, gate = value_ref[...].astype(F32), gate_ref[...].astype(F32)
    gated = value * (1.0 / (1.0 + jnp.exp(-gate)))
    out_ref[...] = gated
    tail_ref[...] = gated[:, gated.shape[1] - tail_ref.shape[1] :]


def diagonal(size):
    rows = lax.broadcasted_iota(jnp.int32, (size, size), 0)
    return rows == lax.broadcasted_iota(jnp.int32, (size, size), 1)


def pack_kernel(weight_ref, taps_ref, out_ref, columns_ref):
    chips, group, width = out_ref.shape
    for i in range(chips):
        out_ref[i] = weight_ref[:, i * width : (i + 1) * width]
    columns_ref[...] = lax.dot_general(
        diagonal(group).astype(F32).astype(BF16),
        taps_ref[...],
        across(1, 1),
        preferred_element_type=F32,
    )


def filter_kernel(head_ref, gated_ref, taps_ref, gain_ref, out_ref):
    line = jnp.concatenate([head_ref[...], gated_ref[...]], axis=1)
    group, tokens = gated_ref.shape
    length, count = line.shape[1], taps_ref.shape[1]
    taps = taps_ref[...]
    total = jnp.zeros((group, tokens), F32)
    for i in range(count):
        begin = length - tokens - (count - 1) + i
        shifted = pltpu.roll(line, (length - begin) % length, 1)[:, :tokens]
        total = total + taps[:, i : i + 1] * shifted
    out_ref[:group, :] = total.astype(BF16)
    gain = jnp.concatenate([gain_ref[...], jnp.zeros((1, tokens - group), F32)], axis=1)
    first = gain.astype(BF16).astype(F32)
    second = (gain - first).astype(BF16).astype(F32)
    third = gain - first - second
    row = lax.broadcasted_iota(jnp.int32, (out_ref.shape[0] - group, tokens), 0)
    extra = jnp.where(row == 0, first, jnp.where(row == 1, second, jnp.where(row == 2, third, 0.0)))
    out_ref[group:, :] = extra.astype(BF16)


def token_kernel(place_ref, rows_ref, own_ref, other_ref, ids_ref, all_ref, upd_ref, send_ref, rank_ref, res_ref, sem):
    chip, core = place_ref[0], place_ref[1]
    blocks, _, _, tokens = rows_ref.shape
    group = own_ref.shape[1]
    half = blocks * group
    width = res_ref.shape[1]
    columns = pl.ds(pl.multiple_of(chip * width, width), width)
    copy = pltpu.make_async_copy(all_ref.at[:, columns], res_ref, sem)
    copy.start()
    both = []
    for which in (core, 1 - core):
        values = rows_ref[:, which, :group].reshape(half, tokens).astype(F32)
        parts = rows_ref[:, which, group:].astype(F32)
        gains = []
        for i in range(blocks):
            line = (parts[i, 0:1] + parts[i, 1:2] + parts[i, 2:3])[:, :group]
            gains.append(jnp.sum(jnp.where(diagonal(group), line, 0.0), axis=1, keepdims=True))
        both.append((values, jnp.concatenate(gains, axis=0)))
    (own, own_gain), (other, other_gain) = both
    channels = 2 * half
    total = jnp.sum(own, axis=0, keepdims=True) + jnp.sum(other, axis=0, keepdims=True)
    squares = jnp.sum(own * own, axis=0, keepdims=True) + jnp.sum(other * other, axis=0, keepdims=True)
    average = total / channels
    variance = squares / channels - average * average
    scale = lax.rsqrt(variance + 1e-05)
    mixed = jnp.zeros((tokens, width), F32)
    for values, gain, weight_ref in ((own, own_gain, own_ref), (other, other_gain, other_ref)):
        weight = weight_ref[...].reshape(half, width)
        normed = (values - average) * scale * gain
        activated = (normed / (1.0 + jnp.exp(-normed))).astype(BF16)
        mixed = mixed + lax.dot_general(
            activated, weight, across(0, 0), preferred_element_type=F32
        )
    copy.wait()
    updated = res_ref[...].astype(F32) + mixed
    mine = width // 2
    upd_ref[...] = jnp.where(core == 0, updated[:, :mine], updated[:, mine:])
    experts, slots = send_ref.shape[:2]
    expert = lax.broadcasted_iota(jnp.int32, (experts, tokens), 0)
    named = (ids_ref[0:1, :] == expert) | (ids_ref[1:2, :] == expert)
    before = lax.broadcasted_iota(jnp.int32, (tokens, tokens), 0)
    after = lax.broadcasted_iota(jnp.int32, (tokens, tokens), 1)
    earlier = jnp.dot(
        named.astype(F32).astype(BF16),
        (before < after).astype(F32).astype(BF16),
        preferred_element_type=F32,
    )
    rank = jnp.where(named, earlier, -1.0)
    rank_ref[...] = rank
    slot = lax.broadcasted_iota(jnp.int32, (experts, slots, tokens), 1) + core * slots
    pick = (rank[:, None, :] == slot.astype(F32)).astype(F32).astype(BF16)
    sent = jnp.dot(
        pick.reshape(experts * slots, tokens), updated.astype(BF16), preferred_element_type=F32
    )
    send_ref[...] = sent.astype(BF16).reshape(experts, slots, width)


def expert_kernel(x_hbm, g0, g1, u0_hbm, u1_hbm, d0_hbm, d1_hbm, out_hbm, *refs):
    x_ref, up_ref, down_ref, out_ref, in_sem, up_sem, down_sem, out_sem = refs
    chunks, _, width = x_hbm.shape
    parts, part = x_ref.shape[0], x_ref.shape[2]
    half = d0_hbm.shape[0]
    ins = [
        pltpu.make_async_copy(x_hbm.at[:, pl.ds(k * part, part)], x_ref.at[k], in_sem.at[k])
        for k in range(parts)
    ]
    ups = [
        pltpu.make_async_copy(w, up_ref.at[k], up_sem.at[k]) for k, w in enumerate((u0_hbm, u1_hbm))
    ]
    downs = [
        pltpu.make_async_copy(w, down_ref.at[pl.ds(k * half, half)], down_sem.at[k])
        for k, w in enumerate((d0_hbm, d1_hbm))
    ]
    ins[0].start()
    ups[0].start()
    ups[1].start()
    outs = []
    for k in range(parts):
        ins[k].wait()
        if k == 0:
            downs[0].start()
            downs[1].start()
            for copy in ins[1:]:
                copy.start()
        x = jnp.concatenate([x_ref[k, i] for i in range(chunks)], axis=1)
        squares = jnp.zeros((part, 1), F32)
        for i in range(chunks):
            piece = x_ref[k, i].astype(F32)
            squares = squares + jnp.sum(piece * piece, axis=1, keepdims=True)
        scale = lax.rsqrt(squares / (chunks * width) + 1e-06)
        gates = [jnp.dot(x, g[...], preferred_element_type=F32) * scale for g in (g0, g1)]
        hidden = []
        for j, gate in enumerate(gates):
            if k == 0:
                ups[j].wait()
            up = jnp.dot(x, up_ref[j], preferred_element_type=F32) * scale
            hidden.append((gate / (1.0 + jnp.exp(-gate)) * up).astype(BF16))
        hidden = jnp.concatenate(hidden, axis=1)
        if k == 0:
            downs[0].wait()
            downs[1].wait()
        for i in range(chunks):
            columns = slice(i * width, (i + 1) * width)
            piece = jnp.dot(hidden, down_ref[:, columns], preferred_element_type=F32)
            out_ref[k, i] = piece.astype(BF16)
        out = pltpu.make_async_copy(out_ref.at[k], out_hbm.at[:, pl.ds(k * part, part)], out_sem.at[k])
        out.start()
        outs.append(out)
    for out in outs:
        out.wait()


def combine_kernel(place_ref, back_ref, rank_ref, ids_ref, w_ref, upd_ref, kept_ref, given_ref):
    core = place_ref[1]
    experts, slots, width = back_ref.shape
    tokens = rank_ref.shape[1]
    expert = lax.broadcasted_iota(jnp.int32, (experts, tokens), 0)
    weight = jnp.where(ids_ref[0:1, :] == expert, w_ref[0:1, :], 0.0) + jnp.where(
        ids_ref[1:2, :] == expert, w_ref[1:2, :], 0.0
    )
    slot = lax.broadcasted_iota(jnp.int32, (experts, slots, tokens), 1) + core * slots
    here = rank_ref[...][:, None, :] == slot.astype(F32)
    spread = jnp.where(here, weight[:, None, :], 0.0).reshape(experts * slots, tokens)
    back = back_ref[...].reshape(experts * slots, width)
    total = jnp.zeros((tokens, width), F32)
    for _ in range(3):
        piece = spread.astype(BF16)
        spread = spread - piece.astype(F32)
        total = total + lax.dot_general(piece, back, across(0, 0), preferred_element_type=F32)
    mine = width // 2
    low, high = total[:, :mine], total[:, mine:]
    kept_ref[...] = upd_ref[...] + jnp.where(core == 0, low, high)
    given_ref[...] = jnp.where(core == 0, high, low)


def local(
    conv_value,
    conv_gate,
    conv_taps,
    conv_gain,
    out_weight,
    residual,
    route_ids,
    route_weight,
    expert_gate,
    expert_up,
    expert_down,
):
    chips, experts = lax.axis_size("y"), lax.axis_size("sp")
    chip, core = lax.axis_index("y"), lax.axis_index("c")
    place = jnp.stack([chip, core]).astype(jnp.int32)
    taps_count, group = conv_taps.shape
    tokens = conv_value.shape[0]
    model = residual.shape[1]
    width = model // chips

    gated, tail = pl.pallas_call(
        gate_kernel,
        out_shape=(pltpu.VMEM((group, tokens), F32), pltpu.VMEM((group, 128), F32)),
        in_specs=[VMEM] * 2,
        out_specs=(VMEM,) * 2,
        compiler_params=room(4),
        name="gate",
    )(far(conv_value.T), far(conv_gate.T))
    tail, out_weight = lax.optimization_barrier((tail, out_weight))
    order = lax.axis_size("sp")
    head = lax.ppermute(tail, "sp", [(i, i + 1) for i in range(order - 1)])
    packed, taps = pl.pallas_call(
        pack_kernel,
        out_shape=(pltpu.VMEM((chips, group, width), BF16), pltpu.VMEM((group, taps_count), F32)),
        in_specs=[VMEM] * 2,
        out_specs=(VMEM,) * 2,
        compiler_params=room(4),
        name="pack",
    )(far(out_weight), far(conv_taps))
    own_out = lax.all_to_all(packed, "y", 0, 0, tiled=True)
    sent = group + 16
    filtered = pl.pallas_call(
        filter_kernel,
        out_shape=pltpu.VMEM((sent, tokens), BF16),
        in_specs=[VMEM] * 4,
        out_specs=VMEM,
        compiler_params=room(4),
        name="filter",
    )(near(head), near(gated), near(taps), far(conv_gain[None]))
    rows = lax.all_gather(filtered, TP, axis=0, tiled=True)
    rows, own_out = lax.optimization_barrier((rows, own_out))
    other_out = twin(own_out)
    rows = rows.reshape(chips, 2, sent, tokens)
    gates = (expert_gate[0], twin(expert_gate[0]))
    ups = (expert_up[0], twin(expert_up[0]))
    downs = (expert_down[0], twin(expert_down[0]))

    ids, weights = route_ids.T, route_weight.T
    slots = 2 * tokens * route_ids.shape[1] // experts // 2
    mine = width // 2
    updated, send, rank = pl.pallas_call(
        token_kernel,
        out_shape=(
            pltpu.VMEM((tokens, mine), F32),
            pltpu.VMEM((experts, slots, width), BF16),
            pltpu.VMEM((experts, tokens), F32),
        ),
        in_specs=[SMEM] + [VMEM] * 4 + [HBM],
        out_specs=(VMEM,) * 3,
        scratch_shapes=[pltpu.VMEM((tokens, width), BF16), pltpu.SemaphoreType.DMA],
        compiler_params=room(12),
        name="token",
    )(place, near(rows), near(own_out), near(other_out), near(ids), far(residual))

    arrived = lax.all_to_all(send, "sp", 0, 0, tiled=True).reshape(1, experts * slots, width)
    full = lax.all_gather(arrived, "y", axis=0, tiled=True)
    parts, part = 2, full.shape[1] // 2
    partial = pl.pallas_call(
        expert_kernel,
        out_shape=pltpu.HBM(full.shape, BF16),
        in_specs=[HBM] + [VMEM] * 2 + [HBM] * 4,
        out_specs=HBM,
        scratch_shapes=[
            pltpu.VMEM((parts, chips, part, width), BF16),
            pltpu.VMEM((2, *ups[0].shape), BF16),
            pltpu.VMEM((2 * downs[0].shape[0], model), BF16),
            pltpu.VMEM((parts, chips, part, width), BF16),
            pltpu.SemaphoreType.DMA((parts,)),
            pltpu.SemaphoreType.DMA((2,)),
            pltpu.SemaphoreType.DMA((2,)),
            pltpu.SemaphoreType.DMA((parts,)),
        ],
        compiler_params=room(32),
        name="expert",
    )(far(full), *(near(w) for w in gates), *(far(w) for w in (*ups, *downs)))
    summed = lax.psum_scatter(partial, "y", scatter_dimension=0, tiled=True)
    back = lax.all_to_all(summed.reshape(experts, slots, width), "sp", 0, 0, tiled=True)
    kept, given = pl.pallas_call(
        combine_kernel,
        out_shape=(pltpu.VMEM((tokens, mine), F32), pltpu.VMEM((tokens, mine), F32)),
        in_specs=[SMEM] + [VMEM] * 5,
        out_specs=(VMEM,) * 2,
        compiler_params=room(8),
        name="combine",
    )(place, near(back), near(rank), near(ids), near(weights), near(updated))
    return (kept + twin(given)).astype(BF16)


def solution(mesh):
    grid = Mesh(mesh.devices.reshape(mesh.shape["sp"], 8, 2), ("sp", "y", "c"))
    placed = (
        P("sp", TP),
        P("sp", TP),
        P(None, TP),
        P(TP),
        P(TP, None),
        P("sp", None),
        P("sp", None),
        P("sp", None),
        P("sp", None, TP),
        P("sp", None, TP),
        P("sp", TP, None),
    )

    return jax.shard_map(local, mesh=grid, in_specs=placed, out_specs=P("sp", TP), check_vma=False)
```

```python
import jax
import jax.numpy as jnp
from jax import lax
from jax.experimental import pallas as pl
from jax.experimental.pallas import tpu as pltpu
from jax.sharding import Mesh
from jax.sharding import PartitionSpec as P

TP = ("y", "c")
VMEM = pl.BlockSpec(memory_space=pltpu.VMEM)
SMEM = pl.BlockSpec(memory_space=pltpu.SMEM)
HBM = pl.BlockSpec(memory_space=pltpu.HBM)
F32 = jnp.float32
BF16 = jnp.bfloat16


def twin(value):
    return lax.ppermute(value, "c", [(0, 1), (1, 0)])


def across(contract_left, contract_right):
    return (((contract_left,), (contract_right,)), ((), ()))


def room(mebibytes):
    return pltpu.CompilerParams(vmem_limit_bytes=mebibytes << 20)


def near(value):
    return pltpu.with_memory_space_constraint(value, pltpu.VMEM)


def far(value):
    return pltpu.with_memory_space_constraint(value, pltpu.HBM)


def gate_kernel(value_ref, gate_ref, out_ref, tail_ref):
    value, gate = value_ref[...].astype(F32), gate_ref[...].astype(F32)
    gated = value * (1.0 / (1.0 + jnp.exp(-gate)))
    out_ref[...] = gated
    tail_ref[...] = gated[:, gated.shape[1] - tail_ref.shape[1] :]


def diagonal(size):
    rows = lax.broadcasted_iota(jnp.int32, (size, size), 0)
    return rows == lax.broadcasted_iota(jnp.int32, (size, size), 1)


def pack_kernel(weight_ref, taps_ref, out_ref, columns_ref):
    receivers, group, width = out_ref.shape
    for i in range(receivers):
        out_ref[i] = weight_ref[:, i // 2 * width : (i // 2 + 1) * width]
    columns_ref[...] = lax.dot_general(
        diagonal(group).astype(F32).astype(BF16),
        taps_ref[...],
        across(1, 1),
        preferred_element_type=F32,
    )


def filter_kernel(head_ref, gated_ref, taps_ref, gain_ref, out_ref):
    line = jnp.concatenate([head_ref[...], gated_ref[...]], axis=1)
    group, tokens = gated_ref.shape
    length, count = line.shape[1], taps_ref.shape[1]
    taps = taps_ref[...]
    total = jnp.zeros((group, tokens), F32)
    for i in range(count):
        begin = length - tokens - (count - 1) + i
        shifted = pltpu.roll(line, (length - begin) % length, 1)[:, :tokens]
        total = total + taps[:, i : i + 1] * shifted
    out_ref[:group, :] = total.astype(BF16)
    gain = jnp.concatenate([gain_ref[...], jnp.zeros((1, tokens - group), F32)], axis=1)
    first = gain.astype(BF16).astype(F32)
    second = (gain - first).astype(BF16).astype(F32)
    third = gain - first - second
    row = lax.broadcasted_iota(jnp.int32, (out_ref.shape[0] - group, tokens), 0)
    extra = jnp.where(row == 0, first, jnp.where(row == 1, second, jnp.where(row == 2, third, 0.0)))
    out_ref[group:, :] = extra.astype(BF16)


def token_kernel(place_ref, rows_ref, weight_ref, ids_ref, all_ref, upd_ref, send_ref, rank_ref, res_ref, sem):
    chip, core = place_ref[0], place_ref[1]
    blocks, _, _, tokens = rows_ref.shape
    group = weight_ref.shape[2]
    half = blocks * group
    width = res_ref.shape[1]
    columns = pl.ds(pl.multiple_of(chip * width, width), width)
    copy = pltpu.make_async_copy(all_ref.at[:, columns], res_ref, sem)
    copy.start()
    both = []
    for which in (0, 1):
        values = rows_ref[:, which, :group].reshape(half, tokens).astype(F32)
        parts = rows_ref[:, which, group:].astype(F32)
        gains = []
        for i in range(blocks):
            line = (parts[i, 0:1] + parts[i, 1:2] + parts[i, 2:3])[:, :group]
            gains.append(jnp.sum(jnp.where(diagonal(group), line, 0.0), axis=1, keepdims=True))
        both.append((values, jnp.concatenate(gains, axis=0)))
    (own, _), (other, _) = both
    channels = 2 * half
    total = jnp.sum(own, axis=0, keepdims=True) + jnp.sum(other, axis=0, keepdims=True)
    squares = jnp.sum(own * own, axis=0, keepdims=True) + jnp.sum(other * other, axis=0, keepdims=True)
    average = total / channels
    variance = squares / channels - average * average
    scale = lax.rsqrt(variance + 1e-05)
    mixed = jnp.zeros((tokens, width), F32)
    for which, (values, gain) in enumerate(both):
        weight = weight_ref[:, which].reshape(half, width)
        normed = (values - average) * scale * gain
        activated = (normed / (1.0 + jnp.exp(-normed))).astype(BF16)
        mixed = mixed + lax.dot_general(
            activated, weight, across(0, 0), preferred_element_type=F32
        )
    copy.wait()
    updated = res_ref[...].astype(F32) + mixed
    mine = width // 2
    upd_ref[...] = jnp.where(core == 0, updated[:, :mine], updated[:, mine:])
    experts, slots = send_ref.shape[:2]
    expert = lax.broadcasted_iota(jnp.int32, (experts, tokens), 0)
    named = (ids_ref[0:1, :] == expert) | (ids_ref[1:2, :] == expert)
    before = lax.broadcasted_iota(jnp.int32, (tokens, tokens), 0)
    after = lax.broadcasted_iota(jnp.int32, (tokens, tokens), 1)
    earlier = jnp.dot(
        named.astype(F32).astype(BF16),
        (before < after).astype(F32).astype(BF16),
        preferred_element_type=F32,
    )
    rank = jnp.where(named, earlier, -1.0)
    rank_ref[...] = rank
    slot = lax.broadcasted_iota(jnp.int32, (experts, slots, tokens), 1) + core * slots
    pick = (rank[:, None, :] == slot.astype(F32)).astype(F32).astype(BF16)
    sent = jnp.dot(
        pick.reshape(experts * slots, tokens), updated.astype(BF16), preferred_element_type=F32
    )
    send_ref[...] = sent.astype(BF16).reshape(experts, slots, width)


def expert_kernel(x_hbm, g0, g1, u0_hbm, u1_hbm, d0_hbm, d1_hbm, out_hbm, *refs):
    x_ref, up_ref, down_ref, out_ref, in_sem, up_sem, down_sem, out_sem = refs
    chunks, _, width = x_hbm.shape
    parts, part = x_ref.shape[0], x_ref.shape[2]
    half = d0_hbm.shape[0]
    ins = [
        pltpu.make_async_copy(x_hbm.at[:, pl.ds(k * part, part)], x_ref.at[k], in_sem.at[k])
        for k in range(parts)
    ]
    ups = [
        pltpu.make_async_copy(w, up_ref.at[k], up_sem.at[k]) for k, w in enumerate((u0_hbm, u1_hbm))
    ]
    downs = [
        pltpu.make_async_copy(w, down_ref.at[pl.ds(k * half, half)], down_sem.at[k])
        for k, w in enumerate((d0_hbm, d1_hbm))
    ]
    ins[0].start()
    outs = []
    for k in range(parts):
        ins[k].wait()
        if k == 0:
            for copy in (*ups, *downs, *ins[1:]):
                copy.start()
        x = jnp.concatenate([x_ref[k, i] for i in range(chunks)], axis=1)
        squares = jnp.zeros((part, 1), F32)
        for i in range(chunks):
            piece = x_ref[k, i].astype(F32)
            squares = squares + jnp.sum(piece * piece, axis=1, keepdims=True)
        scale = lax.rsqrt(squares / (chunks * width) + 1e-06)
        gates = [jnp.dot(x, g[...], preferred_element_type=F32) * scale for g in (g0, g1)]
        hidden = []
        for j, gate in enumerate(gates):
            if k == 0:
                ups[j].wait()
            up = jnp.dot(x, up_ref[j], preferred_element_type=F32) * scale
            hidden.append((gate / (1.0 + jnp.exp(-gate)) * up).astype(BF16))
        hidden = jnp.concatenate(hidden, axis=1)
        if k == 0:
            downs[0].wait()
            downs[1].wait()
        for i in range(chunks):
            columns = slice(i * width, (i + 1) * width)
            piece = jnp.dot(hidden, down_ref[:, columns], preferred_element_type=F32)
            out_ref[k, i] = piece.astype(BF16)
        out = pltpu.make_async_copy(out_ref.at[k], out_hbm.at[:, pl.ds(k * part, part)], out_sem.at[k])
        out.start()
        outs.append(out)
    for out in outs:
        out.wait()


def combine_kernel(place_ref, back_ref, rank_ref, ids_ref, w_ref, upd_ref, kept_ref, given_ref):
    core = place_ref[1]
    experts, slots, width = back_ref.shape
    tokens = rank_ref.shape[1]
    expert = lax.broadcasted_iota(jnp.int32, (experts, tokens), 0)
    weight = jnp.where(ids_ref[0:1, :] == expert, w_ref[0:1, :], 0.0) + jnp.where(
        ids_ref[1:2, :] == expert, w_ref[1:2, :], 0.0
    )
    slot = lax.broadcasted_iota(jnp.int32, (experts, slots, tokens), 1) + core * slots
    here = rank_ref[...][:, None, :] == slot.astype(F32)
    spread = jnp.where(here, weight[:, None, :], 0.0).reshape(experts * slots, tokens)
    back = back_ref[...].reshape(experts * slots, width)
    total = jnp.zeros((tokens, width), F32)
    for _ in range(3):
        piece = spread.astype(BF16)
        spread = spread - piece.astype(F32)
        total = total + lax.dot_general(piece, back, across(0, 0), preferred_element_type=F32)
    mine = width // 2
    low, high = total[:, :mine], total[:, mine:]
    kept_ref[...] = upd_ref[...] + jnp.where(core == 0, low, high)
    given_ref[...] = jnp.where(core == 0, high, low)


def local(
    conv_value,
    conv_gate,
    conv_taps,
    conv_gain,
    out_weight,
    residual,
    route_ids,
    route_weight,
    expert_gate,
    expert_up,
    expert_down,
):
    chips, experts = lax.axis_size("y"), lax.axis_size("sp")
    chip, core = lax.axis_index("y"), lax.axis_index("c")
    place = jnp.stack([chip, core]).astype(jnp.int32)
    taps_count, group = conv_taps.shape
    tokens = conv_value.shape[0]
    model = residual.shape[1]
    width = model // chips

    gated, tail = pl.pallas_call(
        gate_kernel,
        out_shape=(pltpu.VMEM((group, tokens), F32), pltpu.VMEM((group, 128), F32)),
        in_specs=[VMEM] * 2,
        out_specs=(VMEM,) * 2,
        compiler_params=room(4),
        name="gate",
    )(far(conv_value.T), far(conv_gate.T))
    tail, out_weight = lax.optimization_barrier((tail, out_weight))
    order = lax.axis_size("sp")
    head = lax.ppermute(tail, "sp", [(i, i + 1) for i in range(order - 1)])
    packed, taps = pl.pallas_call(
        pack_kernel,
        out_shape=(pltpu.VMEM((2 * chips, group, width), BF16), pltpu.VMEM((group, taps_count), F32)),
        in_specs=[VMEM] * 2,
        out_specs=(VMEM,) * 2,
        compiler_params=room(4),
        name="pack",
    )(far(out_weight), far(conv_taps))
    columns = lax.all_to_all(packed, TP, 0, 0, tiled=True)
    sent = group + 16
    filtered = pl.pallas_call(
        filter_kernel,
        out_shape=pltpu.VMEM((sent, tokens), BF16),
        in_specs=[VMEM] * 4,
        out_specs=VMEM,
        compiler_params=room(4),
        name="filter",
    )(near(head), near(gated), near(taps), far(conv_gain[None]))
    rows = lax.all_gather(filtered, TP, axis=0, tiled=True)
    rows, columns = lax.optimization_barrier((rows, columns))
    rows = rows.reshape(chips, 2, sent, tokens)
    columns = columns.reshape(chips, 2, group, width)
    gates = (expert_gate[0], twin(expert_gate[0]))
    ups = (expert_up[0], twin(expert_up[0]))
    downs = (expert_down[0], twin(expert_down[0]))

    ids, weights = route_ids.T, route_weight.T
    slots = 2 * tokens * route_ids.shape[1] // experts // 2
    mine = width // 2
    updated, send, rank = pl.pallas_call(
        token_kernel,
        out_shape=(
            pltpu.VMEM((tokens, mine), F32),
            pltpu.VMEM((experts, slots, width), BF16),
            pltpu.VMEM((experts, tokens), F32),
        ),
        in_specs=[SMEM] + [VMEM] * 3 + [HBM],
        out_specs=(VMEM,) * 3,
        scratch_shapes=[pltpu.VMEM((tokens, width), BF16), pltpu.SemaphoreType.DMA],
        compiler_params=room(12),
        name="token",
    )(place, near(rows), near(columns), far(ids), far(residual))

    arrived = lax.all_to_all(send, "sp", 0, 0, tiled=True).reshape(1, experts * slots, width)
    full = lax.all_gather(arrived, "y", axis=0, tiled=True)
    parts, part = 2, full.shape[1] // 2
    partial = pl.pallas_call(
        expert_kernel,
        out_shape=pltpu.HBM(full.shape, BF16),
        in_specs=[HBM] + [VMEM] * 2 + [HBM] * 4,
        out_specs=HBM,
        scratch_shapes=[
            pltpu.VMEM((parts, chips, part, width), BF16),
            pltpu.VMEM((2, *ups[0].shape), BF16),
            pltpu.VMEM((2 * downs[0].shape[0], model), BF16),
            pltpu.VMEM((parts, chips, part, width), BF16),
            pltpu.SemaphoreType.DMA((parts,)),
            pltpu.SemaphoreType.DMA((2,)),
            pltpu.SemaphoreType.DMA((2,)),
            pltpu.SemaphoreType.DMA((parts,)),
        ],
        compiler_params=room(32),
        name="expert",
    )(far(full), *(near(w) for w in gates), *(far(w) for w in (*ups, *downs)))
    summed = lax.psum_scatter(partial, "y", scatter_dimension=0, tiled=True)
    back = lax.all_to_all(summed.reshape(experts, slots, width), "sp", 0, 0, tiled=True)
    kept, given = pl.pallas_call(
        combine_kernel,
        out_shape=(pltpu.VMEM((tokens, mine), F32), pltpu.VMEM((tokens, mine), F32)),
        in_specs=[SMEM] + [VMEM] * 5,
        out_specs=(VMEM,) * 2,
        compiler_params=room(8),
        name="combine",
    )(place, near(back), near(rank), near(ids), near(weights), near(updated))
    return (kept + twin(given)).astype(BF16)


def solution(mesh):
    grid = Mesh(mesh.devices.reshape(mesh.shape["sp"], 8, 2), ("sp", "y", "c"))
    placed = (
        P("sp", TP),
        P("sp", TP),
        P(None, TP),
        P(TP),
        P(TP, None),
        P("sp", None),
        P("sp", None),
        P("sp", None),
        P("sp", None, TP),
        P("sp", None, TP),
        P("sp", TP, None),
    )

    return jax.shard_map(local, mesh=grid, in_specs=placed, out_specs=P("sp", TP), check_vma=False)
```

```python
import jax
import jax.numpy as jnp
from jax import lax
from jax.experimental import pallas as pl
from jax.experimental.pallas import tpu as pltpu
from jax.sharding import Mesh
from jax.sharding import PartitionSpec as P

TP = ("y", "c")
VMEM = pl.BlockSpec(memory_space=pltpu.VMEM)
SMEM = pl.BlockSpec(memory_space=pltpu.SMEM)
HBM = pl.BlockSpec(memory_space=pltpu.HBM)
F32 = jnp.float32
BF16 = jnp.bfloat16


def twin(value):
    return lax.ppermute(value, "c", [(0, 1), (1, 0)])


def across(contract_left, contract_right):
    return (((contract_left,), (contract_right,)), ((), ()))


def room(mebibytes):
    return pltpu.CompilerParams(vmem_limit_bytes=mebibytes << 20)


def near(value):
    return pltpu.with_memory_space_constraint(value, pltpu.VMEM)


def far(value):
    return pltpu.with_memory_space_constraint(value, pltpu.HBM)


def gate_kernel(value_ref, gate_ref, out_ref, tail_ref):
    value, gate = value_ref[...].astype(F32), gate_ref[...].astype(F32)
    gated = value * (1.0 / (1.0 + jnp.exp(-gate)))
    out_ref[...] = gated
    tail_ref[...] = gated[:, gated.shape[1] - tail_ref.shape[1] :]


def diagonal(size):
    rows = lax.broadcasted_iota(jnp.int32, (size, size), 0)
    return rows == lax.broadcasted_iota(jnp.int32, (size, size), 1)


def pack_kernel(weight_hbm, taps_ref, gain_ref, out_hbm, columns_ref, rows_ref, sems):
    chips, group, width = out_hbm.shape
    copies = [
        pltpu.make_async_copy(
            weight_hbm.at[:, pl.ds(i * width, width)], out_hbm.at[i], sems.at[i]
        )
        for i in range(chips)
    ]
    for copy in copies:
        copy.start()
    columns_ref[...] = lax.dot_general(
        diagonal(group).astype(F32).astype(BF16),
        taps_ref[...],
        across(1, 1),
        preferred_element_type=F32,
    )
    tokens = rows_ref.shape[1]
    gain = jnp.concatenate([gain_ref[...], jnp.zeros((1, tokens - group), F32)], axis=1)
    first = gain.astype(BF16).astype(F32)
    second = (gain - first).astype(BF16).astype(F32)
    third = gain - first - second
    row = lax.broadcasted_iota(jnp.int32, rows_ref.shape, 0)
    extra = jnp.where(row == 0, first, jnp.where(row == 1, second, jnp.where(row == 2, third, 0.0)))
    rows_ref[...] = extra.astype(BF16)
    for copy in copies:
        copy.wait()


def filter_kernel(head_ref, gated_ref, taps_ref, gain_ref, out_ref):
    line = jnp.concatenate([head_ref[...], gated_ref[...]], axis=1)
    group, tokens = gated_ref.shape
    length, count = line.shape[1], taps_ref.shape[1]
    taps = taps_ref[...]
    total = jnp.zeros((group, tokens), F32)
    for i in range(count):
        begin = length - tokens - (count - 1) + i
        shifted = pltpu.roll(line, (length - begin) % length, 1)[:, :tokens]
        total = total + taps[:, i : i + 1] * shifted
    out_ref[:group, :] = total.astype(BF16)
    out_ref[group:, :] = gain_ref[...]


def token_kernel(place_ref, rows_ref, own_ref, other_ref, ids_ref, all_ref, upd_ref, send_ref, rank_ref, res_ref, sem):
    chip, core = place_ref[0], place_ref[1]
    blocks, _, _, tokens = rows_ref.shape
    group = own_ref.shape[1]
    half = blocks * group
    width = res_ref.shape[1]
    columns = pl.ds(pl.multiple_of(chip * width, width), width)
    copy = pltpu.make_async_copy(all_ref.at[:, columns], res_ref, sem)
    copy.start()
    both = []
    for which in (core, 1 - core):
        values = rows_ref[:, which, :group].reshape(half, tokens).astype(F32)
        parts = rows_ref[:, which, group:].astype(F32)
        gains = []
        for i in range(blocks):
            line = (parts[i, 0:1] + parts[i, 1:2] + parts[i, 2:3])[:, :group]
            gains.append(jnp.sum(jnp.where(diagonal(group), line, 0.0), axis=1, keepdims=True))
        both.append((values, jnp.concatenate(gains, axis=0)))
    (own, own_gain), (other, other_gain) = both
    channels = 2 * half
    total = jnp.sum(own, axis=0, keepdims=True) + jnp.sum(other, axis=0, keepdims=True)
    squares = jnp.sum(own * own, axis=0, keepdims=True) + jnp.sum(other * other, axis=0, keepdims=True)
    average = total / channels
    variance = squares / channels - average * average
    scale = lax.rsqrt(variance + 1e-05)
    mixed = jnp.zeros((tokens, width), F32)
    for values, gain, weight_ref in ((own, own_gain, own_ref), (other, other_gain, other_ref)):
        weight = weight_ref[...].reshape(half, width)
        normed = (values - average) * scale * gain
        activated = (normed / (1.0 + jnp.exp(-normed))).astype(BF16)
        mixed = mixed + lax.dot_general(
            activated, weight, across(0, 0), preferred_element_type=F32
        )
    copy.wait()
    updated = res_ref[...].astype(F32) + mixed
    mine = width // 2
    upd_ref[...] = jnp.where(core == 0, updated[:, :mine], updated[:, mine:])
    experts, slots = send_ref.shape[:2]
    expert = lax.broadcasted_iota(jnp.int32, (experts, tokens), 0)
    named = (ids_ref[0:1, :] == expert) | (ids_ref[1:2, :] == expert)
    before = lax.broadcasted_iota(jnp.int32, (tokens, tokens), 0)
    after = lax.broadcasted_iota(jnp.int32, (tokens, tokens), 1)
    earlier = jnp.dot(
        named.astype(F32).astype(BF16),
        (before < after).astype(F32).astype(BF16),
        preferred_element_type=F32,
    )
    rank = jnp.where(named, earlier, -1.0)
    rank_ref[...] = rank
    slot = lax.broadcasted_iota(jnp.int32, (experts, slots, tokens), 1) + core * slots
    pick = (rank[:, None, :] == slot.astype(F32)).astype(F32).astype(BF16)
    sent = jnp.dot(
        pick.reshape(experts * slots, tokens), updated.astype(BF16), preferred_element_type=F32
    )
    send_ref[...] = sent.astype(BF16).reshape(experts, slots, width)


def expert_kernel(x_hbm, g0, g1, u0_hbm, u1_hbm, d0_hbm, d1_hbm, out_hbm, *refs):
    x_ref, up_ref, down_ref, out_ref, in_sem, up_sem, down_sem, out_sem = refs
    chunks, _, width = x_hbm.shape
    parts, part = x_ref.shape[0], x_ref.shape[2]
    half = d0_hbm.shape[0]
    ins = [
        pltpu.make_async_copy(x_hbm.at[:, pl.ds(k * part, part)], x_ref.at[k], in_sem.at[k])
        for k in range(parts)
    ]
    ups = [
        pltpu.make_async_copy(w, up_ref.at[k], up_sem.at[k]) for k, w in enumerate((u0_hbm, u1_hbm))
    ]
    downs = [
        pltpu.make_async_copy(w, down_ref.at[pl.ds(k * half, half)], down_sem.at[k])
        for k, w in enumerate((d0_hbm, d1_hbm))
    ]
    ins[0].start()
    ups[0].start()
    ups[1].start()
    outs = []
    for k in range(parts):
        ins[k].wait()
        if k == 0:
            downs[0].start()
            downs[1].start()
            for copy in ins[1:]:
                copy.start()
        x = jnp.concatenate([x_ref[k, i] for i in range(chunks)], axis=1)
        squares = jnp.zeros((part, 1), F32)
        for i in range(chunks):
            piece = x_ref[k, i].astype(F32)
            squares = squares + jnp.sum(piece * piece, axis=1, keepdims=True)
        scale = lax.rsqrt(squares / (chunks * width) + 1e-06)
        gates = [jnp.dot(x, g[...], preferred_element_type=F32) * scale for g in (g0, g1)]
        hidden = []
        for j, gate in enumerate(gates):
            if k == 0:
                ups[j].wait()
            up = jnp.dot(x, up_ref[j], preferred_element_type=F32) * scale
            hidden.append((gate / (1.0 + jnp.exp(-gate)) * up).astype(BF16))
        hidden = jnp.concatenate(hidden, axis=1)
        if k == 0:
            downs[0].wait()
            downs[1].wait()
        for i in range(chunks):
            columns = slice(i * width, (i + 1) * width)
            piece = jnp.dot(hidden, down_ref[:, columns], preferred_element_type=F32)
            out_ref[k, i] = piece.astype(BF16)
        out = pltpu.make_async_copy(out_ref.at[k], out_hbm.at[:, pl.ds(k * part, part)], out_sem.at[k])
        out.start()
        outs.append(out)
    for out in outs:
        out.wait()


def combine_kernel(place_ref, back_ref, rank_ref, ids_ref, w_ref, upd_ref, kept_ref, given_ref):
    core = place_ref[1]
    experts, slots, width = back_ref.shape
    tokens = rank_ref.shape[1]
    expert = lax.broadcasted_iota(jnp.int32, (experts, tokens), 0)
    weight = jnp.where(ids_ref[0:1, :] == expert, w_ref[0:1, :], 0.0) + jnp.where(
        ids_ref[1:2, :] == expert, w_ref[1:2, :], 0.0
    )
    slot = lax.broadcasted_iota(jnp.int32, (experts, slots, tokens), 1) + core * slots
    here = rank_ref[...][:, None, :] == slot.astype(F32)
    spread = jnp.where(here, weight[:, None, :], 0.0).reshape(experts * slots, tokens)
    back = back_ref[...].reshape(experts * slots, width)
    total = jnp.zeros((tokens, width), F32)
    for _ in range(3):
        piece = spread.astype(BF16)
        spread = spread - piece.astype(F32)
        total = total + lax.dot_general(piece, back, across(0, 0), preferred_element_type=F32)
    mine = width // 2
    low, high = total[:, :mine], total[:, mine:]
    kept_ref[...] = upd_ref[...] + jnp.where(core == 0, low, high)
    given_ref[...] = jnp.where(core == 0, high, low)


def local(
    conv_value,
    conv_gate,
    conv_taps,
    conv_gain,
    out_weight,
    residual,
    route_ids,
    route_weight,
    expert_gate,
    expert_up,
    expert_down,
):
    chips, experts = lax.axis_size("y"), lax.axis_size("sp")
    chip, core = lax.axis_index("y"), lax.axis_index("c")
    place = jnp.stack([chip, core]).astype(jnp.int32)
    taps_count, group = conv_taps.shape
    tokens = conv_value.shape[0]
    model = residual.shape[1]
    width = model // chips

    gated, tail = pl.pallas_call(
        gate_kernel,
        out_shape=(pltpu.VMEM((group, tokens), F32), pltpu.VMEM((group, 128), F32)),
        in_specs=[VMEM] * 2,
        out_specs=(VMEM,) * 2,
        compiler_params=room(4),
        name="gate",
    )(far(conv_value.T), far(conv_gate.T))
    tail, out_weight = lax.optimization_barrier((tail, out_weight))
    order = lax.axis_size("sp")
    head = lax.ppermute(tail, "sp", [(i, i + 1) for i in range(order - 1)])
    packed, taps, gains = pl.pallas_call(
        pack_kernel,
        out_shape=(
            pltpu.HBM((chips, group, width), BF16),
            pltpu.VMEM((group, taps_count), F32),
            pltpu.VMEM((16, tokens), BF16),
        ),
        in_specs=[HBM, VMEM, VMEM],
        out_specs=(HBM, VMEM, VMEM),
        scratch_shapes=[pltpu.SemaphoreType.DMA((chips,))],
        compiler_params=room(4),
        name="pack",
    )(far(out_weight), far(conv_taps), far(conv_gain[None]))
    own_out = lax.all_to_all(packed, "y", 0, 0, tiled=True)
    sent = group + gains.shape[0]
    filtered = pl.pallas_call(
        filter_kernel,
        out_shape=pltpu.VMEM((sent, tokens), BF16),
        in_specs=[VMEM] * 4,
        out_specs=VMEM,
        compiler_params=room(4),
        name="filter",
    )(near(head), near(gated), near(taps), near(gains))
    rows = lax.all_gather(filtered, TP, axis=0, tiled=True)
    rows, own_out = lax.optimization_barrier((rows, own_out))
    other_out = twin(own_out)
    rows = rows.reshape(chips, 2, sent, tokens)
    gates = (expert_gate[0], twin(expert_gate[0]))
    ups = (expert_up[0], twin(expert_up[0]))
    downs = (expert_down[0], twin(expert_down[0]))

    ids, weights = route_ids.T, route_weight.T
    slots = 2 * tokens * route_ids.shape[1] // experts // 2
    mine = width // 2
    updated, send, rank = pl.pallas_call(
        token_kernel,
        out_shape=(
            pltpu.VMEM((tokens, mine), F32),
            pltpu.VMEM((experts, slots, width), BF16),
            pltpu.VMEM((experts, tokens), F32),
        ),
        in_specs=[SMEM] + [VMEM] * 4 + [HBM],
        out_specs=(VMEM,) * 3,
        scratch_shapes=[pltpu.VMEM((tokens, width), BF16), pltpu.SemaphoreType.DMA],
        compiler_params=room(12),
        name="token",
    )(place, near(rows), near(own_out), near(other_out), far(ids), far(residual))

    arrived = lax.all_to_all(send, "sp", 0, 0, tiled=True).reshape(1, experts * slots, width)
    full = lax.all_gather(arrived, "y", axis=0, tiled=True)
    parts, part = 2, full.shape[1] // 2
    partial = pl.pallas_call(
        expert_kernel,
        out_shape=pltpu.HBM(full.shape, BF16),
        in_specs=[HBM] + [VMEM] * 2 + [HBM] * 4,
        out_specs=HBM,
        scratch_shapes=[
            pltpu.VMEM((parts, chips, part, width), BF16),
            pltpu.VMEM((2, *ups[0].shape), BF16),
            pltpu.VMEM((2 * downs[0].shape[0], model), BF16),
            pltpu.VMEM((parts, chips, part, width), BF16),
            pltpu.SemaphoreType.DMA((parts,)),
            pltpu.SemaphoreType.DMA((2,)),
            pltpu.SemaphoreType.DMA((2,)),
            pltpu.SemaphoreType.DMA((parts,)),
        ],
        compiler_params=room(32),
        name="expert",
    )(far(full), *(near(w) for w in gates), *(far(w) for w in (*ups, *downs)))
    summed = lax.psum_scatter(partial, "y", scatter_dimension=0, tiled=True)
    back = lax.all_to_all(summed.reshape(experts, slots, width), "sp", 0, 0, tiled=True)
    kept, given = pl.pallas_call(
        combine_kernel,
        out_shape=(pltpu.VMEM((tokens, mine), F32), pltpu.VMEM((tokens, mine), F32)),
        in_specs=[SMEM] + [VMEM] * 5,
        out_specs=(VMEM,) * 2,
        compiler_params=room(8),
        name="combine",
    )(place, near(back), near(rank), near(ids), near(weights), near(updated))
    return (kept + twin(given)).astype(BF16)


def solution(mesh):
    grid = Mesh(mesh.devices.reshape(mesh.shape["sp"], 8, 2), ("sp", "y", "c"))
    placed = (
        P("sp", TP),
        P("sp", TP),
        P(None, TP),
        P(TP),
        P(TP, None),
        P("sp", None),
        P("sp", None),
        P("sp", None),
        P("sp", None, TP),
        P("sp", None, TP),
        P("sp", TP, None),
    )

    return jax.shard_map(local, mesh=grid, in_specs=placed, out_specs=P("sp", TP), check_vma=False)
```

```python
import jax
import jax.numpy as jnp
from jax import lax
from jax.experimental import pallas as pl
from jax.experimental.pallas import tpu as pltpu
from jax.sharding import Mesh
from jax.sharding import PartitionSpec as P

TP = ("y", "c")
VMEM = pl.BlockSpec(memory_space=pltpu.VMEM)
SMEM = pl.BlockSpec(memory_space=pltpu.SMEM)
HBM = pl.BlockSpec(memory_space=pltpu.HBM)
F32 = jnp.float32
BF16 = jnp.bfloat16


def twin(value):
    return lax.ppermute(value, "c", [(0, 1), (1, 0)])


def across(contract_left, contract_right):
    return (((contract_left,), (contract_right,)), ((), ()))


def room(mebibytes):
    return pltpu.CompilerParams(vmem_limit_bytes=mebibytes << 20)


def near(value):
    return pltpu.with_memory_space_constraint(value, pltpu.VMEM)


def far(value):
    return pltpu.with_memory_space_constraint(value, pltpu.HBM)


def gate_kernel(value_ref, gate_ref, out_ref, tail_ref):
    value, gate = value_ref[...].astype(F32), gate_ref[...].astype(F32)
    gated = value * (1.0 / (1.0 + jnp.exp(-gate)))
    out_ref[...] = gated
    tail_ref[...] = gated[:, gated.shape[1] - tail_ref.shape[1] :]


def diagonal(size):
    rows = lax.broadcasted_iota(jnp.int32, (size, size), 0)
    return rows == lax.broadcasted_iota(jnp.int32, (size, size), 1)


def pack_kernel(weight_ref, taps_ref, gain_ref, out_ref, columns_ref, rows_ref):
    chips, group, width = out_ref.shape
    for i in range(chips):
        out_ref[i] = weight_ref[:, i * width : (i + 1) * width]
    columns_ref[...] = lax.dot_general(
        diagonal(group).astype(F32).astype(BF16),
        taps_ref[...],
        across(1, 1),
        preferred_element_type=F32,
    )
    tokens = rows_ref.shape[1]
    gain = jnp.concatenate([gain_ref[...], jnp.zeros((1, tokens - group), F32)], axis=1)
    first = gain.astype(BF16).astype(F32)
    second = (gain - first).astype(BF16).astype(F32)
    third = gain - first - second
    row = lax.broadcasted_iota(jnp.int32, rows_ref.shape, 0)
    extra = jnp.where(row == 0, first, jnp.where(row == 1, second, jnp.where(row == 2, third, 0.0)))
    rows_ref[...] = extra.astype(BF16)


def filter_kernel(head_ref, gated_ref, taps_ref, gain_ref, out_ref):
    line = jnp.concatenate([head_ref[...], gated_ref[...]], axis=1)
    group, tokens = gated_ref.shape
    length, count = line.shape[1], taps_ref.shape[1]
    taps = taps_ref[...]
    total = jnp.zeros((group, tokens), F32)
    for i in range(count):
        begin = length - tokens - (count - 1) + i
        shifted = pltpu.roll(line, (length - begin) % length, 1)[:, :tokens]
        total = total + taps[:, i : i + 1] * shifted
    out_ref[:group, :] = total.astype(BF16)
    out_ref[group:, :] = gain_ref[...]


def token_kernel(place_ref, rows_ref, own_ref, other_ref, ids_ref, all_ref, upd_ref, send_ref, rank_ref, res_ref, sem):
    chip, core = place_ref[0], place_ref[1]
    blocks, _, _, tokens = rows_ref.shape
    group = own_ref.shape[1]
    half = blocks * group
    width = res_ref.shape[1]
    columns = pl.ds(pl.multiple_of(chip * width, width), width)
    copy = pltpu.make_async_copy(all_ref.at[:, columns], res_ref, sem)
    copy.start()
    both = []
    for which in (core, 1 - core):
        values = rows_ref[:, which, :group].reshape(half, tokens).astype(F32)
        parts = rows_ref[:, which, group:].astype(F32)
        gains = []
        for i in range(blocks):
            line = (parts[i, 0:1] + parts[i, 1:2] + parts[i, 2:3])[:, :group]
            gains.append(jnp.sum(jnp.where(diagonal(group), line, 0.0), axis=1, keepdims=True))
        both.append((values, jnp.concatenate(gains, axis=0)))
    (own, own_gain), (other, other_gain) = both
    channels = 2 * half
    total = jnp.sum(own, axis=0, keepdims=True) + jnp.sum(other, axis=0, keepdims=True)
    squares = jnp.sum(own * own, axis=0, keepdims=True) + jnp.sum(other * other, axis=0, keepdims=True)
    average = total / channels
    variance = squares / channels - average * average
    scale = lax.rsqrt(variance + 1e-05)
    mixed = jnp.zeros((tokens, width), F32)
    for values, gain, weight_ref in ((own, own_gain, own_ref), (other, other_gain, other_ref)):
        weight = weight_ref[...].reshape(half, width)
        normed = (values - average) * scale * gain
        activated = (normed / (1.0 + jnp.exp(-normed))).astype(BF16)
        mixed = mixed + lax.dot_general(
            activated, weight, across(0, 0), preferred_element_type=F32
        )
    copy.wait()
    updated = res_ref[...].astype(F32) + mixed
    mine = width // 2
    upd_ref[...] = jnp.where(core == 0, updated[:, :mine], updated[:, mine:])
    experts, slots = send_ref.shape[:2]
    expert = lax.broadcasted_iota(jnp.int32, (experts, tokens), 0)
    named = (ids_ref[0:1, :] == expert) | (ids_ref[1:2, :] == expert)
    before = lax.broadcasted_iota(jnp.int32, (tokens, tokens), 0)
    after = lax.broadcasted_iota(jnp.int32, (tokens, tokens), 1)
    earlier = jnp.dot(
        named.astype(F32).astype(BF16),
        (before < after).astype(F32).astype(BF16),
        preferred_element_type=F32,
    )
    rank = jnp.where(named, earlier, -1.0)
    rank_ref[...] = rank
    slot = lax.broadcasted_iota(jnp.int32, (experts, slots, tokens), 1) + core * slots
    pick = (rank[:, None, :] == slot.astype(F32)).astype(F32).astype(BF16)
    sent = jnp.dot(
        pick.reshape(experts * slots, tokens), updated.astype(BF16), preferred_element_type=F32
    )
    send_ref[...] = sent.astype(BF16).reshape(experts, slots, width)


def expert_kernel(x_hbm, g0, g1, u0_hbm, u1_hbm, d0_hbm, d1_hbm, out_hbm, *refs):
    x_ref, up_ref, down_ref, out_ref, in_sem, up_sem, down_sem, out_sem = refs
    chunks, _, width = x_hbm.shape
    parts, part = x_ref.shape[0], x_ref.shape[2]
    half = d0_hbm.shape[0]
    ins = [
        pltpu.make_async_copy(x_hbm.at[:, pl.ds(k * part, part)], x_ref.at[k], in_sem.at[k])
        for k in range(parts)
    ]
    ups = [
        pltpu.make_async_copy(w, up_ref.at[k], up_sem.at[k]) for k, w in enumerate((u0_hbm, u1_hbm))
    ]
    downs = [
        pltpu.make_async_copy(w, down_ref.at[pl.ds(k * half, half)], down_sem.at[k])
        for k, w in enumerate((d0_hbm, d1_hbm))
    ]
    ins[0].start()
    ups[0].start()
    ups[1].start()
    outs = []
    for k in range(parts):
        ins[k].wait()
        if k == 0:
            downs[0].start()
            downs[1].start()
            for copy in ins[1:]:
                copy.start()
        x = jnp.concatenate([x_ref[k, i] for i in range(chunks)], axis=1)
        squares = jnp.zeros((part, 1), F32)
        for i in range(chunks):
            piece = x_ref[k, i].astype(F32)
            squares = squares + jnp.sum(piece * piece, axis=1, keepdims=True)
        scale = lax.rsqrt(squares / (chunks * width) + 1e-06)
        gates = [jnp.dot(x, g[...], preferred_element_type=F32) * scale for g in (g0, g1)]
        hidden = []
        for j, gate in enumerate(gates):
            if k == 0:
                ups[j].wait()
            up = jnp.dot(x, up_ref[j], preferred_element_type=F32) * scale
            hidden.append((gate / (1.0 + jnp.exp(-gate)) * up).astype(BF16))
        hidden = jnp.concatenate(hidden, axis=1)
        if k == 0:
            downs[0].wait()
            downs[1].wait()
        for i in range(chunks):
            columns = slice(i * width, (i + 1) * width)
            piece = jnp.dot(hidden, down_ref[:, columns], preferred_element_type=F32)
            out_ref[k, i] = piece.astype(BF16)
        out = pltpu.make_async_copy(out_ref.at[k], out_hbm.at[:, pl.ds(k * part, part)], out_sem.at[k])
        out.start()
        outs.append(out)
    for out in outs:
        out.wait()


def combine_kernel(place_ref, back_ref, rank_ref, ids_ref, w_ref, upd_ref, kept_ref, given_ref):
    core = place_ref[1]
    experts, slots, width = back_ref.shape
    tokens = rank_ref.shape[1]
    expert = lax.broadcasted_iota(jnp.int32, (experts, tokens), 0)
    weight = jnp.where(ids_ref[0:1, :] == expert, w_ref[0:1, :], 0.0) + jnp.where(
        ids_ref[1:2, :] == expert, w_ref[1:2, :], 0.0
    )
    slot = lax.broadcasted_iota(jnp.int32, (experts, slots, tokens), 1) + core * slots
    here = rank_ref[...][:, None, :] == slot.astype(F32)
    spread = jnp.where(here, weight[:, None, :], 0.0).reshape(experts * slots, tokens)
    back = back_ref[...].reshape(experts * slots, width)
    total = jnp.zeros((tokens, width), F32)
    for _ in range(3):
        piece = spread.astype(BF16)
        spread = spread - piece.astype(F32)
        total = total + lax.dot_general(piece, back, across(0, 0), preferred_element_type=F32)
    mine = width // 2
    low, high = total[:, :mine], total[:, mine:]
    kept_ref[...] = upd_ref[...] + jnp.where(core == 0, low, high)
    given_ref[...] = jnp.where(core == 0, high, low)


def local(
    conv_value,
    conv_gate,
    conv_taps,
    conv_gain,
    out_weight,
    residual,
    route_ids,
    route_weight,
    expert_gate,
    expert_up,
    expert_down,
):
    chips, experts = lax.axis_size("y"), lax.axis_size("sp")
    chip, core = lax.axis_index("y"), lax.axis_index("c")
    place = jnp.stack([chip, core]).astype(jnp.int32)
    taps_count, group = conv_taps.shape
    tokens = conv_value.shape[0]
    model = residual.shape[1]
    width = model // chips

    gated, tail = pl.pallas_call(
        gate_kernel,
        out_shape=(pltpu.VMEM((group, tokens), F32), pltpu.VMEM((group, 128), F32)),
        in_specs=[VMEM] * 2,
        out_specs=(VMEM,) * 2,
        compiler_params=room(4),
        name="gate",
    )(far(conv_value.T), far(conv_gate.T))
    order = lax.axis_size("sp")
    head = lax.ppermute(tail, "sp", [(i, i + 1) for i in range(order - 1)])
    packed, taps, gains = pl.pallas_call(
        pack_kernel,
        out_shape=(
            pltpu.VMEM((chips, group, width), BF16),
            pltpu.VMEM((group, taps_count), F32),
            pltpu.VMEM((16, tokens), BF16),
        ),
        in_specs=[VMEM] * 3,
        out_specs=(VMEM,) * 3,
        compiler_params=room(4),
        name="pack",
    )(far(out_weight), far(conv_taps), far(conv_gain[None]))
    own_out = lax.all_to_all(packed, "y", 0, 0, tiled=True)
    sent = group + gains.shape[0]
    filtered = pl.pallas_call(
        filter_kernel,
        out_shape=pltpu.VMEM((sent, tokens), BF16),
        in_specs=[VMEM] * 4,
        out_specs=VMEM,
        compiler_params=room(4),
        name="filter",
    )(near(head), near(gated), near(taps), near(gains))
    rows = lax.all_gather(filtered, TP, axis=0, tiled=True)
    other_out = twin(own_out)
    rows = rows.reshape(chips, 2, sent, tokens)
    gates = (expert_gate[0], twin(expert_gate[0]))
    ups = (expert_up[0], twin(expert_up[0]))
    downs = (expert_down[0], twin(expert_down[0]))

    ids, weights = route_ids.T, route_weight.T
    slots = 2 * tokens * route_ids.shape[1] // experts // 2
    mine = width // 2
    updated, send, rank = pl.pallas_call(
        token_kernel,
        out_shape=(
            pltpu.VMEM((tokens, mine), F32),
            pltpu.VMEM((experts, slots, width), BF16),
            pltpu.VMEM((experts, tokens), F32),
        ),
        in_specs=[SMEM] + [VMEM] * 4 + [HBM],
        out_specs=(VMEM,) * 3,
        scratch_shapes=[pltpu.VMEM((tokens, width), BF16), pltpu.SemaphoreType.DMA],
        compiler_params=room(12),
        name="token",
    )(place, near(rows), near(own_out), near(other_out), far(ids), far(residual))

    arrived = lax.all_to_all(send, "sp", 0, 0, tiled=True).reshape(1, experts * slots, width)
    full = lax.all_gather(arrived, "y", axis=0, tiled=True)
    parts, part = 2, full.shape[1] // 2
    partial = pl.pallas_call(
        expert_kernel,
        out_shape=pltpu.HBM(full.shape, BF16),
        in_specs=[HBM] + [VMEM] * 2 + [HBM] * 4,
        out_specs=HBM,
        scratch_shapes=[
            pltpu.VMEM((parts, chips, part, width), BF16),
            pltpu.VMEM((2, *ups[0].shape), BF16),
            pltpu.VMEM((2 * downs[0].shape[0], model), BF16),
            pltpu.VMEM((parts, chips, part, width), BF16),
            pltpu.SemaphoreType.DMA((parts,)),
            pltpu.SemaphoreType.DMA((2,)),
            pltpu.SemaphoreType.DMA((2,)),
            pltpu.SemaphoreType.DMA((parts,)),
        ],
        compiler_params=room(32),
        name="expert",
    )(far(full), *(near(w) for w in gates), *(far(w) for w in (*ups, *downs)))
    summed = lax.psum_scatter(partial, "y", scatter_dimension=0, tiled=True)
    back = lax.all_to_all(summed.reshape(experts, slots, width), "sp", 0, 0, tiled=True)
    kept, given = pl.pallas_call(
        combine_kernel,
        out_shape=(pltpu.VMEM((tokens, mine), F32), pltpu.VMEM((tokens, mine), F32)),
        in_specs=[SMEM] + [VMEM] * 5,
        out_specs=(VMEM,) * 2,
        compiler_params=room(8),
        name="combine",
    )(place, near(back), near(rank), near(ids), near(weights), near(updated))
    return (kept + twin(given)).astype(BF16)


def solution(mesh):
    grid = Mesh(mesh.devices.reshape(mesh.shape["sp"], 8, 2), ("sp", "y", "c"))
    placed = (
        P("sp", TP),
        P("sp", TP),
        P(None, TP),
        P(TP),
        P(TP, None),
        P("sp", None),
        P("sp", None),
        P("sp", None),
        P("sp", None, TP),
        P("sp", None, TP),
        P("sp", TP, None),
    )

    return jax.shard_map(local, mesh=grid, in_specs=placed, out_specs=P("sp", TP), check_vma=False)
```

```python
import jax
import jax.numpy as jnp
from jax import lax
from jax.experimental import pallas as pl
from jax.experimental.pallas import tpu as pltpu
from jax.sharding import Mesh
from jax.sharding import PartitionSpec as P

TP = ("y", "c")
VMEM = pl.BlockSpec(memory_space=pltpu.VMEM)
SMEM = pl.BlockSpec(memory_space=pltpu.SMEM)
HBM = pl.BlockSpec(memory_space=pltpu.HBM)
F32 = jnp.float32
BF16 = jnp.bfloat16


def twin(value):
    return lax.ppermute(value, "c", [(0, 1), (1, 0)])


def across(contract_left, contract_right):
    return (((contract_left,), (contract_right,)), ((), ()))


def room(mebibytes):
    return pltpu.CompilerParams(vmem_limit_bytes=mebibytes << 20)


def near(value):
    return pltpu.with_memory_space_constraint(value, pltpu.VMEM)


def far(value):
    return pltpu.with_memory_space_constraint(value, pltpu.HBM)


def diagonal(size):
    rows = lax.broadcasted_iota(jnp.int32, (size, size), 0)
    return rows == lax.broadcasted_iota(jnp.int32, (size, size), 1)


def first_kernel(
    value_ref, gate_ref, weight_ref, taps_ref, gain_ref, gated_ref, tail_ref, out_ref, columns_ref, rows_ref
):
    value, gate = value_ref[...].astype(F32), gate_ref[...].astype(F32)
    gated = value * (1.0 / (1.0 + jnp.exp(-gate)))
    gated_ref[...] = gated
    tail_ref[...] = gated[:, gated.shape[1] - tail_ref.shape[1] :]
    chips, group, width = out_ref.shape
    for i in range(chips):
        out_ref[i] = weight_ref[:, i * width : (i + 1) * width]
    columns_ref[...] = lax.dot_general(
        diagonal(group).astype(F32).astype(BF16),
        taps_ref[...],
        across(1, 1),
        preferred_element_type=F32,
    )
    tokens = rows_ref.shape[1]
    gain = jnp.concatenate([gain_ref[...], jnp.zeros((1, tokens - group), F32)], axis=1)
    first = gain.astype(BF16).astype(F32)
    second = (gain - first).astype(BF16).astype(F32)
    third = gain - first - second
    row = lax.broadcasted_iota(jnp.int32, rows_ref.shape, 0)
    extra = jnp.where(row == 0, first, jnp.where(row == 1, second, jnp.where(row == 2, third, 0.0)))
    rows_ref[...] = extra.astype(BF16)


def filter_kernel(head_ref, gated_ref, taps_ref, gain_ref, out_ref):
    line = jnp.concatenate([head_ref[...], gated_ref[...]], axis=1)
    group, tokens = gated_ref.shape
    length, count = line.shape[1], taps_ref.shape[1]
    taps = taps_ref[...]
    total = jnp.zeros((group, tokens), F32)
    for i in range(count):
        begin = length - tokens - (count - 1) + i
        shifted = pltpu.roll(line, (length - begin) % length, 1)[:, :tokens]
        total = total + taps[:, i : i + 1] * shifted
    out_ref[:group, :] = total.astype(BF16)
    out_ref[group:, :] = gain_ref[...]


def token_kernel(
    place_ref, rows_ref, own_ref, other_ref, ids_hbm, all_ref, upd_ref, send_ref, rank_ref, res_ref, ids_ref, sem, ids_sem
):
    chip, core = place_ref[0], place_ref[1]
    blocks, _, _, tokens = rows_ref.shape
    group = own_ref.shape[1]
    half = blocks * group
    width = res_ref.shape[1]
    columns = pl.ds(pl.multiple_of(chip * width, width), width)
    copy = pltpu.make_async_copy(all_ref.at[:, columns], res_ref, sem)
    copy.start()
    ids_copy = pltpu.make_async_copy(ids_hbm, ids_ref, ids_sem)
    ids_copy.start()
    both = []
    for which in (core, 1 - core):
        values = rows_ref[:, which, :group].reshape(half, tokens).astype(F32)
        parts = rows_ref[:, which, group:].astype(F32)
        gains = []
        for i in range(blocks):
            line = (parts[i, 0:1] + parts[i, 1:2] + parts[i, 2:3])[:, :group]
            gains.append(jnp.sum(jnp.where(diagonal(group), line, 0.0), axis=1, keepdims=True))
        both.append((values, jnp.concatenate(gains, axis=0)))
    (own, own_gain), (other, other_gain) = both
    channels = 2 * half
    total = jnp.sum(own, axis=0, keepdims=True) + jnp.sum(other, axis=0, keepdims=True)
    squares = jnp.sum(own * own, axis=0, keepdims=True) + jnp.sum(other * other, axis=0, keepdims=True)
    average = total / channels
    variance = squares / channels - average * average
    scale = lax.rsqrt(variance + 1e-05)
    mixed = jnp.zeros((tokens, width), F32)
    for values, gain, weight_ref in ((own, own_gain, own_ref), (other, other_gain, other_ref)):
        weight = weight_ref[...].reshape(half, width)
        normed = (values - average) * scale * gain
        activated = (normed / (1.0 + jnp.exp(-normed))).astype(BF16)
        mixed = mixed + lax.dot_general(
            activated, weight, across(0, 0), preferred_element_type=F32
        )
    copy.wait()
    updated = res_ref[...].astype(F32) + mixed
    mine = width // 2
    upd_ref[...] = jnp.where(core == 0, updated[:, :mine], updated[:, mine:])
    ids_copy.wait()
    experts, slots = send_ref.shape[:2]
    expert = lax.broadcasted_iota(jnp.int32, (experts, tokens), 0)
    named = (ids_ref[0:1, :] == expert) | (ids_ref[1:2, :] == expert)
    before = lax.broadcasted_iota(jnp.int32, (tokens, tokens), 0)
    after = lax.broadcasted_iota(jnp.int32, (tokens, tokens), 1)
    earlier = jnp.dot(
        named.astype(F32).astype(BF16),
        (before < after).astype(F32).astype(BF16),
        preferred_element_type=F32,
    )
    rank = jnp.where(named, earlier, -1.0)
    rank_ref[...] = rank
    slot = lax.broadcasted_iota(jnp.int32, (experts, slots, tokens), 1) + core * slots
    pick = (rank[:, None, :] == slot.astype(F32)).astype(F32).astype(BF16)
    sent = jnp.dot(
        pick.reshape(experts * slots, tokens), updated.astype(BF16), preferred_element_type=F32
    )
    send_ref[...] = sent.astype(BF16).reshape(experts, slots, width)


def expert_kernel(x_hbm, g0, g1, u0_hbm, u1_hbm, d0_hbm, d1_hbm, out_hbm, *refs):
    x_ref, up_ref, down_ref, out_ref, in_sem, up_sem, down_sem, out_sem = refs
    chunks, _, width = x_hbm.shape
    parts, part = x_ref.shape[0], x_ref.shape[2]
    half = d0_hbm.shape[0]
    ins = [
        pltpu.make_async_copy(x_hbm.at[:, pl.ds(k * part, part)], x_ref.at[k], in_sem.at[k])
        for k in range(parts)
    ]
    ups = [
        pltpu.make_async_copy(w, up_ref.at[k], up_sem.at[k]) for k, w in enumerate((u0_hbm, u1_hbm))
    ]
    downs = [
        pltpu.make_async_copy(w, down_ref.at[pl.ds(k * half, half)], down_sem.at[k])
        for k, w in enumerate((d0_hbm, d1_hbm))
    ]
    ins[0].start()
    ups[0].start()
    ups[1].start()
    outs = []
    for k in range(parts):
        ins[k].wait()
        if k == 0:
            downs[0].start()
            downs[1].start()
            for copy in ins[1:]:
                copy.start()
        x = jnp.concatenate([x_ref[k, i] for i in range(chunks)], axis=1)
        squares = jnp.zeros((part, width), F32)
        for i in range(chunks):
            piece = x_ref[k, i].astype(F32)
            squares = squares + piece * piece
        squares = jnp.sum(squares, axis=1, keepdims=True)
        scale = lax.rsqrt(squares / (chunks * width) + 1e-06)
        gates = [jnp.dot(x, g[...], preferred_element_type=F32) * scale for g in (g0, g1)]
        hidden = []
        for j, gate in enumerate(gates):
            if k == 0:
                ups[j].wait()
            up = jnp.dot(x, up_ref[j], preferred_element_type=F32) * scale
            hidden.append((gate / (1.0 + jnp.exp(-gate)) * up).astype(BF16))
        hidden = jnp.concatenate(hidden, axis=1)
        if k == 0:
            downs[0].wait()
            downs[1].wait()
        for i in range(chunks):
            columns = slice(i * width, (i + 1) * width)
            piece = jnp.dot(hidden, down_ref[:, columns], preferred_element_type=F32)
            out_ref[k, i] = piece.astype(BF16)
        out = pltpu.make_async_copy(out_ref.at[k], out_hbm.at[:, pl.ds(k * part, part)], out_sem.at[k])
        out.start()
        outs.append(out)
    for out in outs:
        out.wait()


def combine_kernel(place_ref, back_ref, rank_ref, ids_ref, w_ref, upd_ref, kept_ref, given_ref):
    core = place_ref[1]
    experts, slots, width = back_ref.shape
    tokens = rank_ref.shape[1]
    expert = lax.broadcasted_iota(jnp.int32, (experts, tokens), 0)
    weight = jnp.where(ids_ref[0:1, :] == expert, w_ref[0:1, :], 0.0) + jnp.where(
        ids_ref[1:2, :] == expert, w_ref[1:2, :], 0.0
    )
    slot = lax.broadcasted_iota(jnp.int32, (experts, slots, tokens), 1) + core * slots
    here = rank_ref[...][:, None, :] == slot.astype(F32)
    spread = jnp.where(here, weight[:, None, :], 0.0).reshape(experts * slots, tokens)
    back = back_ref[...].reshape(experts * slots, width)
    total = jnp.zeros((tokens, width), F32)
    for _ in range(3):
        piece = spread.astype(BF16)
        spread = spread - piece.astype(F32)
        total = total + lax.dot_general(piece, back, across(0, 0), preferred_element_type=F32)
    mine = width // 2
    low, high = total[:, :mine], total[:, mine:]
    kept_ref[...] = upd_ref[...] + jnp.where(core == 0, low, high)
    given_ref[...] = jnp.where(core == 0, high, low)


def local(
    conv_value,
    conv_gate,
    conv_taps,
    conv_gain,
    out_weight,
    residual,
    route_ids,
    route_weight,
    expert_gate,
    expert_up,
    expert_down,
):
    chips, experts = lax.axis_size("y"), lax.axis_size("sp")
    chip, core = lax.axis_index("y"), lax.axis_index("c")
    place = jnp.stack([chip, core]).astype(jnp.int32)
    taps_count, group = conv_taps.shape
    tokens = conv_value.shape[0]
    model = residual.shape[1]
    width = model // chips

    gated, tail, packed, taps, gains = pl.pallas_call(
        first_kernel,
        out_shape=(
            pltpu.VMEM((group, tokens), F32),
            pltpu.VMEM((group, 128), F32),
            pltpu.VMEM((chips, group, width), BF16),
            pltpu.VMEM((group, taps_count), F32),
            pltpu.VMEM((16, tokens), BF16),
        ),
        in_specs=[VMEM] * 5,
        out_specs=(VMEM,) * 5,
        compiler_params=room(4),
        name="first",
    )(*(far(a) for a in (conv_value.T, conv_gate.T, out_weight, conv_taps, conv_gain[None])))
    order = lax.axis_size("sp")
    head = lax.ppermute(tail, "sp", [(i, i + 1) for i in range(order - 1)])
    own_out = lax.all_to_all(packed, "y", 0, 0, tiled=True)
    sent = group + gains.shape[0]
    filtered = pl.pallas_call(
        filter_kernel,
        out_shape=pltpu.VMEM((sent, tokens), BF16),
        in_specs=[VMEM] * 4,
        out_specs=VMEM,
        compiler_params=room(4),
        name="filter",
    )(near(head), near(gated), near(taps), near(gains))
    rows = lax.all_gather(filtered, TP, axis=0, tiled=True)
    other_out = twin(own_out)
    rows = rows.reshape(chips, 2, sent, tokens)
    gates = (expert_gate[0], twin(expert_gate[0]))
    ups = (expert_up[0], twin(expert_up[0]))
    downs = (expert_down[0], twin(expert_down[0]))

    ids, weights = route_ids.T, route_weight.T
    slots = 2 * tokens * route_ids.shape[1] // experts // 2
    mine = width // 2
    updated, send, rank = pl.pallas_call(
        token_kernel,
        out_shape=(
            pltpu.VMEM((tokens, mine), F32),
            pltpu.VMEM((experts, slots, width), BF16),
            pltpu.VMEM((experts, tokens), F32),
        ),
        in_specs=[SMEM] + [VMEM] * 3 + [HBM] * 2,
        out_specs=(VMEM,) * 3,
        scratch_shapes=[
            pltpu.VMEM((tokens, width), BF16),
            pltpu.VMEM(ids.shape, jnp.int32),
            pltpu.SemaphoreType.DMA,
            pltpu.SemaphoreType.DMA,
        ],
        compiler_params=room(12),
        name="token",
    )(place, near(rows), near(own_out), near(other_out), far(ids), far(residual))

    arrived = lax.all_to_all(send, "sp", 0, 0, tiled=True).reshape(1, experts * slots, width)
    full = lax.all_gather(arrived, "y", axis=0, tiled=True)
    parts, part = 2, full.shape[1] // 2
    partial = pl.pallas_call(
        expert_kernel,
        out_shape=pltpu.HBM(full.shape, BF16),
        in_specs=[HBM] + [VMEM] * 2 + [HBM] * 4,
        out_specs=HBM,
        scratch_shapes=[
            pltpu.VMEM((parts, chips, part, width), BF16),
            pltpu.VMEM((2, *ups[0].shape), BF16),
            pltpu.VMEM((2 * downs[0].shape[0], model), BF16),
            pltpu.VMEM((parts, chips, part, width), BF16),
            pltpu.SemaphoreType.DMA((parts,)),
            pltpu.SemaphoreType.DMA((2,)),
            pltpu.SemaphoreType.DMA((2,)),
            pltpu.SemaphoreType.DMA((parts,)),
        ],
        compiler_params=room(32),
        name="expert",
    )(far(full), *(near(w) for w in gates), *(far(w) for w in (*ups, *downs)))
    summed = lax.psum_scatter(partial, "y", scatter_dimension=0, tiled=True)
    back = lax.all_to_all(summed.reshape(experts, slots, width), "sp", 0, 0, tiled=True)
    kept, given = pl.pallas_call(
        combine_kernel,
        out_shape=(pltpu.VMEM((tokens, mine), F32), pltpu.VMEM((tokens, mine), F32)),
        in_specs=[SMEM] + [VMEM] * 5,
        out_specs=(VMEM,) * 2,
        compiler_params=room(8),
        name="combine",
    )(place, near(back), near(rank), near(ids), near(weights), near(updated))
    return (kept + twin(given)).astype(BF16)


def solution(mesh):
    grid = Mesh(mesh.devices.reshape(mesh.shape["sp"], 8, 2), ("sp", "y", "c"))
    placed = (
        P("sp", TP),
        P("sp", TP),
        P(None, TP),
        P(TP),
        P(TP, None),
        P("sp", None),
        P("sp", None),
        P("sp", None),
        P("sp", None, TP),
        P("sp", None, TP),
        P("sp", TP, None),
    )

    return jax.shard_map(local, mesh=grid, in_specs=placed, out_specs=P("sp", TP), check_vma=False)
```

```python
import jax
import jax.numpy as jnp
from jax import lax
from jax.experimental import pallas as pl
from jax.experimental.pallas import tpu as pltpu
from jax.sharding import Mesh
from jax.sharding import PartitionSpec as P

TP = ("y", "c")
VMEM = pl.BlockSpec(memory_space=pltpu.VMEM)
SMEM = pl.BlockSpec(memory_space=pltpu.SMEM)
HBM = pl.BlockSpec(memory_space=pltpu.HBM)
F32 = jnp.float32
BF16 = jnp.bfloat16


def twin(value):
    return lax.ppermute(value, "c", [(0, 1), (1, 0)])


def across(contract_left, contract_right):
    return (((contract_left,), (contract_right,)), ((), ()))


def room(mebibytes):
    return pltpu.CompilerParams(vmem_limit_bytes=mebibytes << 20)


def near(value):
    return pltpu.with_memory_space_constraint(value, pltpu.VMEM)


def far(value):
    return pltpu.with_memory_space_constraint(value, pltpu.HBM)


def diagonal(size):
    rows = lax.broadcasted_iota(jnp.int32, (size, size), 0)
    return rows == lax.broadcasted_iota(jnp.int32, (size, size), 1)


def first_kernel(
    value_ref, gate_ref, weight_ref, taps_ref, gain_ref, gated_ref, tail_ref, out_ref, columns_ref, rows_ref
):
    value, gate = value_ref[...].astype(F32), gate_ref[...].astype(F32)
    gated = value * (1.0 / (1.0 + jnp.exp(-gate)))
    gated_ref[...] = gated
    tail_ref[...] = gated[:, gated.shape[1] - tail_ref.shape[1] :]
    chips, group, width = out_ref.shape
    for i in range(chips):
        out_ref[i] = weight_ref[:, i * width : (i + 1) * width]
    columns_ref[...] = lax.dot_general(
        diagonal(group).astype(F32).astype(BF16),
        taps_ref[...],
        across(1, 1),
        preferred_element_type=F32,
    )
    tokens = rows_ref.shape[1]
    gain = jnp.concatenate([gain_ref[...], jnp.zeros((1, tokens - group), F32)], axis=1)
    first = gain.astype(BF16).astype(F32)
    second = (gain - first).astype(BF16).astype(F32)
    third = gain - first - second
    row = lax.broadcasted_iota(jnp.int32, rows_ref.shape, 0)
    extra = jnp.where(row == 0, first, jnp.where(row == 1, second, jnp.where(row == 2, third, 0.0)))
    rows_ref[...] = extra.astype(BF16)


def filter_kernel(head_ref, gated_ref, taps_ref, gain_ref, out_ref):
    line = jnp.concatenate([head_ref[...], gated_ref[...]], axis=1)
    group, tokens = gated_ref.shape
    length, count = line.shape[1], taps_ref.shape[1]
    taps = taps_ref[...]
    total = jnp.zeros((group, tokens), F32)
    for i in range(count):
        begin = length - tokens - (count - 1) + i
        shifted = pltpu.roll(line, (length - begin) % length, 1)[:, :tokens]
        total = total + taps[:, i : i + 1] * shifted
    out_ref[:group, :] = total.astype(BF16)
    out_ref[group:, :] = gain_ref[...]


def token_kernel(
    place_ref, rows_ref, own_ref, other_ref, ids_hbm, all_ref, upd_ref, send_ref, rank_ref, res_ref, ids_ref, sem, ids_sem
):
    chip, core = place_ref[0], place_ref[1]
    blocks, _, _, tokens = rows_ref.shape
    group = own_ref.shape[1]
    half = blocks * group
    width = res_ref.shape[1]
    columns = pl.ds(pl.multiple_of(chip * width, width), width)
    copy = pltpu.make_async_copy(all_ref.at[:, columns], res_ref, sem)
    copy.start()
    ids_copy = pltpu.make_async_copy(ids_hbm, ids_ref, ids_sem)
    ids_copy.start()
    both = []
    for which in (core, 1 - core):
        values = rows_ref[:, which, :group].reshape(half, tokens).astype(F32)
        parts = rows_ref[:, which, group:].astype(F32)
        gains = []
        for i in range(blocks):
            line = (parts[i, 0:1] + parts[i, 1:2] + parts[i, 2:3])[:, :group]
            gains.append(jnp.sum(jnp.where(diagonal(group), line, 0.0), axis=1, keepdims=True))
        both.append((values, jnp.concatenate(gains, axis=0)))
    (own, own_gain), (other, other_gain) = both
    channels = 2 * half
    total = jnp.sum(own, axis=0, keepdims=True) + jnp.sum(other, axis=0, keepdims=True)
    squares = jnp.sum(own * own, axis=0, keepdims=True) + jnp.sum(other * other, axis=0, keepdims=True)
    average = total / channels
    variance = squares / channels - average * average
    scale = lax.rsqrt(variance + 1e-05)
    mixed = jnp.zeros((tokens, width), F32)
    for values, gain, weight_ref in ((own, own_gain, own_ref), (other, other_gain, other_ref)):
        weight = weight_ref[...].reshape(half, width)
        normed = (values - average) * scale * gain
        activated = (normed / (1.0 + jnp.exp(-normed))).astype(BF16)
        mixed = mixed + lax.dot_general(
            activated, weight, across(0, 0), preferred_element_type=F32
        )
    copy.wait()
    updated = res_ref[...].astype(F32) + mixed
    mine = width // 2
    upd_ref[...] = jnp.where(core == 0, updated[:, :mine], updated[:, mine:])
    ids_copy.wait()
    experts, slots = send_ref.shape[:2]
    expert = lax.broadcasted_iota(jnp.int32, (experts, tokens), 0)
    named = (ids_ref[0:1, :] == expert) | (ids_ref[1:2, :] == expert)
    before = lax.broadcasted_iota(jnp.int32, (tokens, tokens), 0)
    after = lax.broadcasted_iota(jnp.int32, (tokens, tokens), 1)
    earlier = jnp.dot(
        named.astype(F32).astype(BF16),
        (before < after).astype(F32).astype(BF16),
        preferred_element_type=F32,
    )
    rank = jnp.where(named, earlier, -1.0)
    rank_ref[...] = rank
    slot = lax.broadcasted_iota(jnp.int32, (experts, slots, tokens), 1) + core * slots
    pick = (rank[:, None, :] == slot.astype(F32)).astype(F32).astype(BF16)
    sent = jnp.dot(
        pick.reshape(experts * slots, tokens), updated.astype(BF16), preferred_element_type=F32
    )
    send_ref[...] = sent.astype(BF16).reshape(experts, slots, width)


def expert_kernel(x_hbm, g0, g1, u0_hbm, u1_hbm, d0_hbm, d1_hbm, out_hbm, *refs):
    x_ref, up_ref, down_ref, out_ref, in_sem, up_sem, down_sem, out_sem = refs
    chunks, _, width = x_hbm.shape
    parts, part = x_ref.shape[0], x_ref.shape[2]
    half = d0_hbm.shape[0]
    ins = [
        [
            pltpu.make_async_copy(
                x_hbm.at[i, pl.ds(k * part, part)], x_ref.at[k, i], in_sem.at[k, i]
            )
            for i in range(chunks)
        ]
        for k in range(parts)
    ]
    pieces = up_sem.shape[1]
    step = u0_hbm.shape[0] // pieces
    ups = [
        [
            pltpu.make_async_copy(
                w.at[pl.ds(r * step, step)], up_ref.at[k, pl.ds(r * step, step)], up_sem.at[k, r]
            )
            for r in range(pieces)
        ]
        for k, w in enumerate((u0_hbm, u1_hbm))
    ]
    less = half // pieces
    downs = [
        pltpu.make_async_copy(
            w.at[pl.ds(r * less, less)],
            down_ref.at[pl.ds(k * half + r * less, less)],
            down_sem.at[k, r],
        )
        for k, w in enumerate((d0_hbm, d1_hbm))
        for r in range(pieces)
    ]
    for copy in (*ins[0], *ups[0], *ups[1]):
        copy.start()
    outs = []
    for k in range(parts):
        for copy in ins[k]:
            copy.wait()
        if k == 0:
            for copy in (*downs, *(copy for later in ins[1:] for copy in later)):
                copy.start()
        x = jnp.concatenate([x_ref[k, i] for i in range(chunks)], axis=1)
        squares = jnp.zeros((part, width), F32)
        for i in range(chunks):
            piece = x_ref[k, i].astype(F32)
            squares = squares + piece * piece
        squares = jnp.sum(squares, axis=1, keepdims=True)
        scale = lax.rsqrt(squares / (chunks * width) + 1e-06)
        gates = [jnp.dot(x, g[...], preferred_element_type=F32) * scale for g in (g0, g1)]
        hidden = []
        for j, gate in enumerate(gates):
            if k == 0:
                for copy in ups[j]:
                    copy.wait()
            up = jnp.dot(x, up_ref[j], preferred_element_type=F32) * scale
            hidden.append((gate / (1.0 + jnp.exp(-gate)) * up).astype(BF16))
        hidden = jnp.concatenate(hidden, axis=1)
        if k == 0:
            for copy in downs:
                copy.wait()
        for i in range(chunks):
            columns = slice(i * width, (i + 1) * width)
            piece = jnp.dot(hidden, down_ref[:, columns], preferred_element_type=F32)
            out_ref[k, i] = piece.astype(BF16)
            out = pltpu.make_async_copy(
                out_ref.at[k, i], out_hbm.at[i, pl.ds(k * part, part)], out_sem.at[k, i]
            )
            out.start()
            outs.append(out)
    for out in outs:
        out.wait()


def combine_kernel(place_ref, back_ref, rank_ref, ids_ref, w_ref, upd_ref, kept_ref, given_ref):
    core = place_ref[1]
    experts, slots, width = back_ref.shape
    tokens = rank_ref.shape[1]
    expert = lax.broadcasted_iota(jnp.int32, (experts, tokens), 0)
    weight = jnp.where(ids_ref[0:1, :] == expert, w_ref[0:1, :], 0.0) + jnp.where(
        ids_ref[1:2, :] == expert, w_ref[1:2, :], 0.0
    )
    slot = lax.broadcasted_iota(jnp.int32, (experts, slots, tokens), 1) + core * slots
    here = rank_ref[...][:, None, :] == slot.astype(F32)
    spread = jnp.where(here, weight[:, None, :], 0.0).reshape(experts * slots, tokens)
    back = back_ref[...].reshape(experts * slots, width)
    total = jnp.zeros((tokens, width), F32)
    for _ in range(3):
        piece = spread.astype(BF16)
        spread = spread - piece.astype(F32)
        total = total + lax.dot_general(piece, back, across(0, 0), preferred_element_type=F32)
    mine = width // 2
    low, high = total[:, :mine], total[:, mine:]
    kept_ref[...] = upd_ref[...] + jnp.where(core == 0, low, high)
    given_ref[...] = jnp.where(core == 0, high, low)


def local(
    conv_value,
    conv_gate,
    conv_taps,
    conv_gain,
    out_weight,
    residual,
    route_ids,
    route_weight,
    expert_gate,
    expert_up,
    expert_down,
):
    chips, experts = lax.axis_size("y"), lax.axis_size("sp")
    chip, core = lax.axis_index("y"), lax.axis_index("c")
    place = jnp.stack([chip, core]).astype(jnp.int32)
    taps_count, group = conv_taps.shape
    tokens = conv_value.shape[0]
    model = residual.shape[1]
    width = model // chips

    gated, tail, packed, taps, gains = pl.pallas_call(
        first_kernel,
        out_shape=(
            pltpu.VMEM((group, tokens), F32),
            pltpu.VMEM((group, 128), F32),
            pltpu.VMEM((chips, group, width), BF16),
            pltpu.VMEM((group, taps_count), F32),
            pltpu.VMEM((16, tokens), BF16),
        ),
        in_specs=[VMEM] * 5,
        out_specs=(VMEM,) * 5,
        compiler_params=room(4),
        name="first",
    )(*(far(a) for a in (conv_value.T, conv_gate.T, out_weight, conv_taps, conv_gain[None])))
    order = lax.axis_size("sp")
    head = lax.ppermute(tail, "sp", [(i, i + 1) for i in range(order - 1)])
    own_out = lax.all_to_all(packed, "y", 0, 0, tiled=True)
    sent = group + gains.shape[0]
    filtered = pl.pallas_call(
        filter_kernel,
        out_shape=pltpu.VMEM((sent, tokens), BF16),
        in_specs=[VMEM] * 4,
        out_specs=VMEM,
        compiler_params=room(4),
        name="filter",
    )(near(head), near(gated), near(taps), near(gains))
    rows = lax.all_gather(filtered, TP, axis=0, tiled=True)
    other_out = twin(own_out)
    rows = rows.reshape(chips, 2, sent, tokens)
    gates = (expert_gate[0], twin(expert_gate[0]))
    ups = (expert_up[0], twin(expert_up[0]))
    downs = (expert_down[0], twin(expert_down[0]))

    ids, weights = route_ids.T, route_weight.T
    slots = 2 * tokens * route_ids.shape[1] // experts // 2
    mine = width // 2
    updated, send, rank = pl.pallas_call(
        token_kernel,
        out_shape=(
            pltpu.VMEM((tokens, mine), F32),
            pltpu.VMEM((experts, slots, width), BF16),
            pltpu.VMEM((experts, tokens), F32),
        ),
        in_specs=[SMEM] + [VMEM] * 3 + [HBM] * 2,
        out_specs=(VMEM,) * 3,
        scratch_shapes=[
            pltpu.VMEM((tokens, width), BF16),
            pltpu.VMEM(ids.shape, jnp.int32),
            pltpu.SemaphoreType.DMA,
            pltpu.SemaphoreType.DMA,
        ],
        compiler_params=room(12),
        name="token",
    )(place, near(rows), near(own_out), near(other_out), far(ids), far(residual))

    arrived = lax.all_to_all(send, "sp", 0, 0, tiled=True).reshape(1, experts * slots, width)
    full = lax.all_gather(arrived, "y", axis=0, tiled=True)
    parts, part = 1, full.shape[1]
    partial = pl.pallas_call(
        expert_kernel,
        out_shape=pltpu.HBM(full.shape, BF16),
        in_specs=[HBM] + [VMEM] * 2 + [HBM] * 4,
        out_specs=HBM,
        scratch_shapes=[
            pltpu.VMEM((parts, chips, part, width), BF16),
            pltpu.VMEM((2, *ups[0].shape), BF16),
            pltpu.VMEM((2 * downs[0].shape[0], model), BF16),
            pltpu.VMEM((parts, chips, part, width), BF16),
            pltpu.SemaphoreType.DMA((parts, chips)),
            pltpu.SemaphoreType.DMA((2, 4)),
            pltpu.SemaphoreType.DMA((2, 4)),
            pltpu.SemaphoreType.DMA((parts, chips)),
        ],
        compiler_params=room(32),
        name="expert",
    )(far(full), *(near(w) for w in gates), *(far(w) for w in (*ups, *downs)))
    summed = lax.psum_scatter(partial, "y", scatter_dimension=0, tiled=True)
    back = lax.all_to_all(summed.reshape(experts, slots, width), "sp", 0, 0, tiled=True)
    kept, given = pl.pallas_call(
        combine_kernel,
        out_shape=(pltpu.VMEM((tokens, mine), F32), pltpu.VMEM((tokens, mine), F32)),
        in_specs=[SMEM] + [VMEM] * 5,
        out_specs=(VMEM,) * 2,
        compiler_params=room(8),
        name="combine",
    )(place, near(back), near(rank), near(ids), near(weights), near(updated))
    return (kept + twin(given)).astype(BF16)


def solution(mesh):
    grid = Mesh(mesh.devices.reshape(mesh.shape["sp"], 8, 2), ("sp", "y", "c"))
    placed = (
        P("sp", TP),
        P("sp", TP),
        P(None, TP),
        P(TP),
        P(TP, None),
        P("sp", None),
        P("sp", None),
        P("sp", None),
        P("sp", None, TP),
        P("sp", None, TP),
        P("sp", TP, None),
    )

    return jax.shard_map(local, mesh=grid, in_specs=placed, out_specs=P("sp", TP), check_vma=False)
```

```python
import jax
import jax.numpy as jnp
from jax import lax
from jax.experimental import pallas as pl
from jax.experimental.pallas import tpu as pltpu
from jax.sharding import Mesh
from jax.sharding import PartitionSpec as P

TP = ("y", "c")
VMEM = pl.BlockSpec(memory_space=pltpu.VMEM)
SMEM = pl.BlockSpec(memory_space=pltpu.SMEM)
HBM = pl.BlockSpec(memory_space=pltpu.HBM)
F32 = jnp.float32
BF16 = jnp.bfloat16


def twin(value):
    return lax.ppermute(value, "c", [(0, 1), (1, 0)])


def across(contract_left, contract_right):
    return (((contract_left,), (contract_right,)), ((), ()))


def room(mebibytes):
    return pltpu.CompilerParams(vmem_limit_bytes=mebibytes << 20)


def near(value):
    return pltpu.with_memory_space_constraint(value, pltpu.VMEM)


def far(value):
    return pltpu.with_memory_space_constraint(value, pltpu.HBM)


def diagonal(size):
    rows = lax.broadcasted_iota(jnp.int32, (size, size), 0)
    return rows == lax.broadcasted_iota(jnp.int32, (size, size), 1)


def first_kernel(
    value_ref, gate_ref, weight_ref, taps_ref, gain_ref, gated_ref, tail_ref, out_ref, columns_ref, rows_ref
):
    value, gate = value_ref[...].astype(F32), gate_ref[...].astype(F32)
    gated = value * (1.0 / (1.0 + jnp.exp(-gate)))
    gated_ref[...] = gated
    tail_ref[...] = gated[:, gated.shape[1] - tail_ref.shape[1] :]
    chips, group, width = out_ref.shape
    for i in range(chips):
        out_ref[i] = weight_ref[:, i * width : (i + 1) * width]
    columns_ref[...] = lax.dot_general(
        diagonal(group).astype(F32).astype(BF16),
        taps_ref[...],
        across(1, 1),
        preferred_element_type=F32,
    )
    tokens = rows_ref.shape[1]
    gain = jnp.concatenate([gain_ref[...], jnp.zeros((1, tokens - group), F32)], axis=1)
    first = gain.astype(BF16).astype(F32)
    second = (gain - first).astype(BF16).astype(F32)
    third = gain - first - second
    row = lax.broadcasted_iota(jnp.int32, rows_ref.shape, 0)
    extra = jnp.where(row == 0, first, jnp.where(row == 1, second, jnp.where(row == 2, third, 0.0)))
    rows_ref[...] = extra.astype(BF16)


def filter_kernel(head_ref, gated_ref, taps_ref, gain_ref, out_ref):
    line = jnp.concatenate([head_ref[...], gated_ref[...]], axis=1)
    group, tokens = gated_ref.shape
    length, count = line.shape[1], taps_ref.shape[1]
    taps = taps_ref[...]
    total = jnp.zeros((group, tokens), F32)
    for i in range(count):
        begin = length - tokens - (count - 1) + i
        shifted = pltpu.roll(line, (length - begin) % length, 1)[:, :tokens]
        total = total + taps[:, i : i + 1] * shifted
    out_ref[:group, :] = total.astype(BF16)
    out_ref[group:, :] = gain_ref[...]


def token_kernel(
    place_ref, rows_ref, own_ref, other_ref, ids_hbm, all_ref, upd_ref, send_ref, rank_ref, res_ref, ids_ref, sem, ids_sem
):
    chip, core = place_ref[0], place_ref[1]
    blocks, _, _, tokens = rows_ref.shape
    group = own_ref.shape[1]
    half = blocks * group
    width = res_ref.shape[1]
    columns = pl.ds(pl.multiple_of(chip * width, width), width)
    copy = pltpu.make_async_copy(all_ref.at[:, columns], res_ref, sem)
    copy.start()
    ids_copy = pltpu.make_async_copy(ids_hbm, ids_ref, ids_sem)
    ids_copy.start()
    both = []
    for which in (core, 1 - core):
        values = rows_ref[:, which, :group].reshape(half, tokens).astype(F32)
        parts = rows_ref[:, which, group:].astype(F32)
        gains = []
        for i in range(blocks):
            line = (parts[i, 0:1] + parts[i, 1:2] + parts[i, 2:3])[:, :group]
            gains.append(jnp.sum(jnp.where(diagonal(group), line, 0.0), axis=1, keepdims=True))
        both.append((values, jnp.concatenate(gains, axis=0)))
    (own, own_gain), (other, other_gain) = both
    channels = 2 * half
    total = jnp.sum(own, axis=0, keepdims=True) + jnp.sum(other, axis=0, keepdims=True)
    squares = jnp.sum(own * own, axis=0, keepdims=True) + jnp.sum(other * other, axis=0, keepdims=True)
    average = total / channels
    variance = squares / channels - average * average
    scale = lax.rsqrt(variance + 1e-05)
    mixed = jnp.zeros((tokens, width), F32)
    for values, gain, weight_ref in ((own, own_gain, own_ref), (other, other_gain, other_ref)):
        weight = weight_ref[...].reshape(half, width)
        normed = (values - average) * scale * gain
        activated = (normed / (1.0 + jnp.exp(-normed))).astype(BF16)
        mixed = mixed + lax.dot_general(
            activated, weight, across(0, 0), preferred_element_type=F32
        )
    copy.wait()
    updated = res_ref[...].astype(F32) + mixed
    mine = width // 2
    upd_ref[...] = jnp.where(core == 0, updated[:, :mine], updated[:, mine:])
    ids_copy.wait()
    experts, slots = send_ref.shape[:2]
    expert = lax.broadcasted_iota(jnp.int32, (experts, tokens), 0)
    named = (ids_ref[0:1, :] == expert) | (ids_ref[1:2, :] == expert)
    before = lax.broadcasted_iota(jnp.int32, (tokens, tokens), 0)
    after = lax.broadcasted_iota(jnp.int32, (tokens, tokens), 1)
    earlier = jnp.dot(
        named.astype(F32).astype(BF16),
        (before < after).astype(F32).astype(BF16),
        preferred_element_type=F32,
    )
    rank = jnp.where(named, earlier, -1.0)
    rank_ref[...] = rank
    slot = lax.broadcasted_iota(jnp.int32, (experts, slots, tokens), 1) + core * slots
    pick = (rank[:, None, :] == slot.astype(F32)).astype(F32).astype(BF16)
    sent = jnp.dot(
        pick.reshape(experts * slots, tokens), updated.astype(BF16), preferred_element_type=F32
    )
    send_ref[...] = sent.astype(BF16).reshape(experts, slots, width)


def expert_kernel(x_hbm, g0, g1, u0_hbm, u1_hbm, d0_hbm, d1_hbm, out_hbm, *refs):
    x_ref, up_ref, down_ref, out_ref, in_sem, up_sem, down_sem, out_sem = refs
    chunks, _, width = x_hbm.shape
    parts, part = x_ref.shape[0], x_ref.shape[2]
    half = d0_hbm.shape[0]
    ins = [
        pltpu.make_async_copy(x_hbm.at[:, pl.ds(k * part, part)], x_ref.at[k], in_sem.at[k])
        for k in range(parts)
    ]
    ups = [
        pltpu.make_async_copy(w, up_ref.at[k], up_sem.at[k]) for k, w in enumerate((u0_hbm, u1_hbm))
    ]
    downs = [
        pltpu.make_async_copy(w, down_ref.at[pl.ds(k * half, half)], down_sem.at[k])
        for k, w in enumerate((d0_hbm, d1_hbm))
    ]
    ins[0].start()
    ups[0].start()
    ups[1].start()
    outs = []
    for k in range(parts):
        ins[k].wait()
        if k == 0:
            downs[0].start()
            downs[1].start()
            for copy in ins[1:]:
                copy.start()
        x = jnp.concatenate([x_ref[k, i] for i in range(chunks)], axis=1)
        squares = jnp.zeros((part, width), F32)
        for i in range(chunks):
            piece = x_ref[k, i].astype(F32)
            squares = squares + piece * piece
        squares = jnp.sum(squares, axis=1, keepdims=True)
        scale = lax.rsqrt(squares / (chunks * width) + 1e-06)
        gates = [jnp.dot(x, g[...], preferred_element_type=F32) * scale for g in (g0, g1)]
        hidden = []
        for j, gate in enumerate(gates):
            if k == 0:
                ups[j].wait()
            up = jnp.dot(x, up_ref[j], preferred_element_type=F32) * scale
            hidden.append((gate / (1.0 + jnp.exp(-gate)) * up).astype(BF16))
        hidden = jnp.concatenate(hidden, axis=1)
        if k == 0:
            downs[0].wait()
            downs[1].wait()
        for i in range(chunks):
            columns = slice(i * width, (i + 1) * width)
            piece = jnp.dot(hidden, down_ref[:, columns], preferred_element_type=F32)
            out_ref[k, i] = piece.astype(BF16)
            out = pltpu.make_async_copy(
                out_ref.at[k, i], out_hbm.at[i, pl.ds(k * part, part)], out_sem.at[k, i]
            )
            out.start()
            outs.append(out)
    for out in outs:
        out.wait()


def combine_kernel(place_ref, back_ref, rank_ref, ids_ref, w_ref, upd_ref, kept_ref, given_ref):
    core = place_ref[1]
    experts, slots, width = back_ref.shape
    tokens = rank_ref.shape[1]
    expert = lax.broadcasted_iota(jnp.int32, (experts, tokens), 0)
    weight = jnp.where(ids_ref[0:1, :] == expert, w_ref[0:1, :], 0.0) + jnp.where(
        ids_ref[1:2, :] == expert, w_ref[1:2, :], 0.0
    )
    slot = lax.broadcasted_iota(jnp.int32, (experts, slots, tokens), 1) + core * slots
    here = rank_ref[...][:, None, :] == slot.astype(F32)
    spread = jnp.where(here, weight[:, None, :], 0.0).reshape(experts * slots, tokens)
    back = back_ref[...].reshape(experts * slots, width)
    total = jnp.zeros((tokens, width), F32)
    for _ in range(3):
        piece = spread.astype(BF16)
        spread = spread - piece.astype(F32)
        total = total + lax.dot_general(piece, back, across(0, 0), preferred_element_type=F32)
    mine = width // 2
    low, high = total[:, :mine], total[:, mine:]
    kept_ref[...] = upd_ref[...] + jnp.where(core == 0, low, high)
    given_ref[...] = jnp.where(core == 0, high, low)


def local(
    conv_value,
    conv_gate,
    conv_taps,
    conv_gain,
    out_weight,
    residual,
    route_ids,
    route_weight,
    expert_gate,
    expert_up,
    expert_down,
):
    chips, experts = lax.axis_size("y"), lax.axis_size("sp")
    chip, core = lax.axis_index("y"), lax.axis_index("c")
    place = jnp.stack([chip, core]).astype(jnp.int32)
    taps_count, group = conv_taps.shape
    tokens = conv_value.shape[0]
    model = residual.shape[1]
    width = model // chips

    gated, tail, packed, taps, gains = pl.pallas_call(
        first_kernel,
        out_shape=(
            pltpu.VMEM((group, tokens), F32),
            pltpu.VMEM((group, 128), F32),
            pltpu.VMEM((chips, group, width), BF16),
            pltpu.VMEM((group, taps_count), F32),
            pltpu.VMEM((16, tokens), BF16),
        ),
        in_specs=[VMEM] * 5,
        out_specs=(VMEM,) * 5,
        compiler_params=room(4),
        name="first",
    )(*(far(a) for a in (conv_value.T, conv_gate.T, out_weight, conv_taps, conv_gain[None])))
    order = lax.axis_size("sp")
    head = lax.ppermute(tail, "sp", [(i, i + 1) for i in range(order - 1)])
    own_out = lax.all_to_all(packed, "y", 0, 0, tiled=True)
    sent = group + gains.shape[0]
    filtered = pl.pallas_call(
        filter_kernel,
        out_shape=pltpu.VMEM((sent, tokens), BF16),
        in_specs=[VMEM] * 4,
        out_specs=VMEM,
        compiler_params=room(4),
        name="filter",
    )(near(head), near(gated), near(taps), near(gains))
    rows = lax.all_gather(filtered, TP, axis=0, tiled=True)
    other_out = twin(own_out)
    rows = rows.reshape(chips, 2, sent, tokens)
    gates = (expert_gate[0], twin(expert_gate[0]))
    ups = (expert_up[0], twin(expert_up[0]))
    downs = (expert_down[0], twin(expert_down[0]))

    ids, weights = route_ids.T, route_weight.T
    slots = 2 * tokens * route_ids.shape[1] // experts // 2
    mine = width // 2
    updated, send, rank = pl.pallas_call(
        token_kernel,
        out_shape=(
            pltpu.VMEM((tokens, mine), F32),
            pltpu.VMEM((experts, slots, width), BF16),
            pltpu.VMEM((experts, tokens), F32),
        ),
        in_specs=[SMEM] + [VMEM] * 3 + [HBM] * 2,
        out_specs=(VMEM,) * 3,
        scratch_shapes=[
            pltpu.VMEM((tokens, width), BF16),
            pltpu.VMEM(ids.shape, jnp.int32),
            pltpu.SemaphoreType.DMA,
            pltpu.SemaphoreType.DMA,
        ],
        compiler_params=room(12),
        name="token",
    )(place, near(rows), near(own_out), near(other_out), far(ids), far(residual))

    arrived = lax.all_to_all(send, "sp", 0, 0, tiled=True).reshape(1, experts * slots, width)
    full = lax.all_gather(arrived, "y", axis=0, tiled=True)
    parts, part = 2, full.shape[1] // 2
    partial = pl.pallas_call(
        expert_kernel,
        out_shape=pltpu.HBM(full.shape, BF16),
        in_specs=[HBM] + [VMEM] * 2 + [HBM] * 4,
        out_specs=HBM,
        scratch_shapes=[
            pltpu.VMEM((parts, chips, part, width), BF16),
            pltpu.VMEM((2, *ups[0].shape), BF16),
            pltpu.VMEM((2 * downs[0].shape[0], model), BF16),
            pltpu.VMEM((parts, chips, part, width), BF16),
            pltpu.SemaphoreType.DMA((parts,)),
            pltpu.SemaphoreType.DMA((2,)),
            pltpu.SemaphoreType.DMA((2,)),
            pltpu.SemaphoreType.DMA((parts, chips)),
        ],
        compiler_params=room(32),
        name="expert",
    )(far(full), *(near(w) for w in gates), *(far(w) for w in (*ups, *downs)))
    summed = lax.psum_scatter(partial, "y", scatter_dimension=0, tiled=True)
    back = lax.all_to_all(summed.reshape(experts, slots, width), "sp", 0, 0, tiled=True)
    kept, given = pl.pallas_call(
        combine_kernel,
        out_shape=(pltpu.VMEM((tokens, mine), F32), pltpu.VMEM((tokens, mine), F32)),
        in_specs=[SMEM] + [VMEM] * 5,
        out_specs=(VMEM,) * 2,
        compiler_params=room(8),
        name="combine",
    )(place, near(back), near(rank), near(ids), near(weights), near(updated))
    return (kept + twin(given)).astype(BF16)


def solution(mesh):
    grid = Mesh(mesh.devices.reshape(mesh.shape["sp"], 8, 2), ("sp", "y", "c"))
    placed = (
        P("sp", TP),
        P("sp", TP),
        P(None, TP),
        P(TP),
        P(TP, None),
        P("sp", None),
        P("sp", None),
        P("sp", None),
        P("sp", None, TP),
        P("sp", None, TP),
        P("sp", TP, None),
    )

    return jax.shard_map(local, mesh=grid, in_specs=placed, out_specs=P("sp", TP), check_vma=False)
```

```python
import jax
import jax.numpy as jnp
from jax import lax
from jax.experimental import pallas as pl
from jax.experimental.pallas import tpu as pltpu
from jax.sharding import Mesh
from jax.sharding import PartitionSpec as P

TP = ("y", "c")
VMEM = pl.BlockSpec(memory_space=pltpu.VMEM)
SMEM = pl.BlockSpec(memory_space=pltpu.SMEM)
HBM = pl.BlockSpec(memory_space=pltpu.HBM)
F32 = jnp.float32
BF16 = jnp.bfloat16


def twin(value):
    return lax.ppermute(value, "c", [(0, 1), (1, 0)])


def across(contract_left, contract_right):
    return (((contract_left,), (contract_right,)), ((), ()))


def room(mebibytes):
    return pltpu.CompilerParams(vmem_limit_bytes=mebibytes << 20)


def near(value):
    return pltpu.with_memory_space_constraint(value, pltpu.VMEM)


def far(value):
    return pltpu.with_memory_space_constraint(value, pltpu.HBM)


def diagonal(size):
    rows = lax.broadcasted_iota(jnp.int32, (size, size), 0)
    return rows == lax.broadcasted_iota(jnp.int32, (size, size), 1)


def first_kernel(
    value_ref, gate_ref, weight_ref, taps_ref, gain_ref, gated_ref, tail_ref, out_ref, columns_ref, rows_ref
):
    value, gate = value_ref[...].astype(F32), gate_ref[...].astype(F32)
    gated = value * (1.0 / (1.0 + jnp.exp(-gate)))
    gated_ref[...] = gated
    tail_ref[...] = gated[:, gated.shape[1] - tail_ref.shape[1] :]
    chips, group, width = out_ref.shape
    for i in range(chips):
        out_ref[i] = weight_ref[:, i * width : (i + 1) * width]
    columns_ref[...] = lax.dot_general(
        diagonal(group).astype(F32).astype(BF16),
        taps_ref[...],
        across(1, 1),
        preferred_element_type=F32,
    )
    tokens = rows_ref.shape[1]
    gain = jnp.concatenate([gain_ref[...], jnp.zeros((1, tokens - group), F32)], axis=1)
    first = gain.astype(BF16).astype(F32)
    second = (gain - first).astype(BF16).astype(F32)
    third = gain - first - second
    row = lax.broadcasted_iota(jnp.int32, rows_ref.shape, 0)
    extra = jnp.where(row == 0, first, jnp.where(row == 1, second, jnp.where(row == 2, third, 0.0)))
    rows_ref[...] = extra.astype(BF16)


def filter_kernel(head_ref, gated_ref, taps_ref, gain_ref, out_ref):
    line = jnp.concatenate([head_ref[...], gated_ref[...]], axis=1)
    group, tokens = gated_ref.shape
    length, count = line.shape[1], taps_ref.shape[1]
    taps = taps_ref[...]
    total = jnp.zeros((group, tokens), F32)
    for i in range(count):
        begin = length - tokens - (count - 1) + i
        shifted = pltpu.roll(line, (length - begin) % length, 1)[:, :tokens]
        total = total + taps[:, i : i + 1] * shifted
    out_ref[:group, :] = total.astype(BF16)
    out_ref[group:, :] = gain_ref[...]


def plan_kernel(place_ref, ids_ref, all_ref, pick_ref, rank_ref, res_ref, sem):
    chip, core = place_ref[0], place_ref[1]
    width, tokens = res_ref.shape[1], rank_ref.shape[1]
    columns = pl.ds(pl.multiple_of(chip * width, width), width)
    copy = pltpu.make_async_copy(all_ref.at[:, columns], res_ref, sem)
    copy.start()
    experts = rank_ref.shape[0]
    slots = pick_ref.shape[0] // experts
    expert = lax.broadcasted_iota(jnp.int32, (experts, tokens), 0)
    named = (ids_ref[0:1, :] == expert) | (ids_ref[1:2, :] == expert)
    before = lax.broadcasted_iota(jnp.int32, (tokens, tokens), 0)
    after = lax.broadcasted_iota(jnp.int32, (tokens, tokens), 1)
    earlier = jnp.dot(
        named.astype(F32).astype(BF16),
        (before < after).astype(F32).astype(BF16),
        preferred_element_type=F32,
    )
    rank = jnp.where(named, earlier, -1.0)
    rank_ref[...] = rank
    slot = lax.broadcasted_iota(jnp.int32, (experts, slots, tokens), 1) + core * slots
    pick = (rank[:, None, :] == slot.astype(F32)).astype(F32).astype(BF16)
    pick_ref[...] = pick.reshape(experts * slots, tokens)
    copy.wait()


def token_kernel(place_ref, rows_ref, own_ref, other_ref, pick_ref, res_ref, upd_ref, send_ref):
    core = place_ref[1]
    blocks, _, _, tokens = rows_ref.shape
    group = own_ref.shape[1]
    half = blocks * group
    width = res_ref.shape[1]
    both = []
    for which in (core, 1 - core):
        values = rows_ref[:, which, :group].reshape(half, tokens).astype(F32)
        parts = rows_ref[:, which, group:].astype(F32)
        gains = []
        for i in range(blocks):
            line = (parts[i, 0:1] + parts[i, 1:2] + parts[i, 2:3])[:, :group]
            gains.append(jnp.sum(jnp.where(diagonal(group), line, 0.0), axis=1, keepdims=True))
        both.append((values, jnp.concatenate(gains, axis=0)))
    (own, own_gain), (other, other_gain) = both
    channels = 2 * half
    total = jnp.sum(own, axis=0, keepdims=True) + jnp.sum(other, axis=0, keepdims=True)
    squares = jnp.sum(own * own, axis=0, keepdims=True) + jnp.sum(other * other, axis=0, keepdims=True)
    average = total / channels
    variance = squares / channels - average * average
    scale = lax.rsqrt(variance + 1e-05)
    mixed = jnp.zeros((tokens, width), F32)
    for values, gain, weight_ref in ((own, own_gain, own_ref), (other, other_gain, other_ref)):
        weight = weight_ref[...].reshape(half, width)
        normed = (values - average) * scale * gain
        activated = (normed / (1.0 + jnp.exp(-normed))).astype(BF16)
        mixed = mixed + lax.dot_general(
            activated, weight, across(0, 0), preferred_element_type=F32
        )
    updated = res_ref[...].astype(F32) + mixed
    mine = width // 2
    upd_ref[...] = jnp.where(core == 0, updated[:, :mine], updated[:, mine:])
    experts, slots = send_ref.shape[:2]
    sent = jnp.dot(
        pick_ref[...], updated.astype(BF16), preferred_element_type=F32
    )
    send_ref[...] = sent.astype(BF16).reshape(experts, slots, width)


def expert_kernel(x_hbm, g0, g1, u0_hbm, u1_hbm, d0_hbm, d1_hbm, out_hbm, *refs):
    x_ref, up_ref, down_ref, out_ref, in_sem, up_sem, down_sem, out_sem = refs
    chunks, _, width = x_hbm.shape
    parts, part = x_ref.shape[0], x_ref.shape[2]
    half = d0_hbm.shape[0]
    ins = [
        pltpu.make_async_copy(x_hbm.at[:, pl.ds(k * part, part)], x_ref.at[k], in_sem.at[k])
        for k in range(parts)
    ]
    ups = [
        pltpu.make_async_copy(w, up_ref.at[k], up_sem.at[k]) for k, w in enumerate((u0_hbm, u1_hbm))
    ]
    downs = [
        pltpu.make_async_copy(w, down_ref.at[pl.ds(k * half, half)], down_sem.at[k])
        for k, w in enumerate((d0_hbm, d1_hbm))
    ]
    ins[0].start()
    ups[0].start()
    ups[1].start()
    outs = []
    for k in range(parts):
        ins[k].wait()
        if k == 0:
            downs[0].start()
            downs[1].start()
            for copy in ins[1:]:
                copy.start()
        x = jnp.concatenate([x_ref[k, i] for i in range(chunks)], axis=1)
        squares = jnp.zeros((part, width), F32)
        for i in range(chunks):
            piece = x_ref[k, i].astype(F32)
            squares = squares + piece * piece
        squares = jnp.sum(squares, axis=1, keepdims=True)
        scale = lax.rsqrt(squares / (chunks * width) + 1e-06)
        gates = [jnp.dot(x, g[...], preferred_element_type=F32) * scale for g in (g0, g1)]
        hidden = []
        for j, gate in enumerate(gates):
            if k == 0:
                ups[j].wait()
            up = jnp.dot(x, up_ref[j], preferred_element_type=F32) * scale
            hidden.append((gate / (1.0 + jnp.exp(-gate)) * up).astype(BF16))
        hidden = jnp.concatenate(hidden, axis=1)
        if k == 0:
            downs[0].wait()
            downs[1].wait()
        for i in range(chunks):
            columns = slice(i * width, (i + 1) * width)
            piece = jnp.dot(hidden, down_ref[:, columns], preferred_element_type=F32)
            out_ref[k, i] = piece.astype(BF16)
            out = pltpu.make_async_copy(
                out_ref.at[k, i], out_hbm.at[i, pl.ds(k * part, part)], out_sem.at[k, i]
            )
            out.start()
            outs.append(out)
    for out in outs:
        out.wait()


def combine_kernel(place_ref, back_ref, rank_ref, ids_ref, w_ref, upd_ref, kept_ref, given_ref):
    core = place_ref[1]
    experts, slots, width = back_ref.shape
    tokens = rank_ref.shape[1]
    expert = lax.broadcasted_iota(jnp.int32, (experts, tokens), 0)
    weight = jnp.where(ids_ref[0:1, :] == expert, w_ref[0:1, :], 0.0) + jnp.where(
        ids_ref[1:2, :] == expert, w_ref[1:2, :], 0.0
    )
    slot = lax.broadcasted_iota(jnp.int32, (experts, slots, tokens), 1) + core * slots
    here = rank_ref[...][:, None, :] == slot.astype(F32)
    spread = jnp.where(here, weight[:, None, :], 0.0).reshape(experts * slots, tokens)
    back = back_ref[...].reshape(experts * slots, width)
    total = jnp.zeros((tokens, width), F32)
    for _ in range(3):
        piece = spread.astype(BF16)
        spread = spread - piece.astype(F32)
        total = total + lax.dot_general(piece, back, across(0, 0), preferred_element_type=F32)
    mine = width // 2
    low, high = total[:, :mine], total[:, mine:]
    kept_ref[...] = upd_ref[...] + jnp.where(core == 0, low, high)
    given_ref[...] = jnp.where(core == 0, high, low)


def local(
    conv_value,
    conv_gate,
    conv_taps,
    conv_gain,
    out_weight,
    residual,
    route_ids,
    route_weight,
    expert_gate,
    expert_up,
    expert_down,
):
    chips, experts = lax.axis_size("y"), lax.axis_size("sp")
    chip, core = lax.axis_index("y"), lax.axis_index("c")
    place = jnp.stack([chip, core]).astype(jnp.int32)
    taps_count, group = conv_taps.shape
    tokens = conv_value.shape[0]
    model = residual.shape[1]
    width = model // chips

    gated, tail, packed, taps, gains = pl.pallas_call(
        first_kernel,
        out_shape=(
            pltpu.VMEM((group, tokens), F32),
            pltpu.VMEM((group, 128), F32),
            pltpu.VMEM((chips, group, width), BF16),
            pltpu.VMEM((group, taps_count), F32),
            pltpu.VMEM((16, tokens), BF16),
        ),
        in_specs=[VMEM] * 5,
        out_specs=(VMEM,) * 5,
        compiler_params=room(4),
        name="first",
    )(*(far(a) for a in (conv_value.T, conv_gate.T, out_weight, conv_taps, conv_gain[None])))
    ids, weights = route_ids.T, route_weight.T
    slots = 2 * tokens * route_ids.shape[1] // experts // 2
    mine = width // 2
    pick, rank, res = pl.pallas_call(
        plan_kernel,
        out_shape=(
            pltpu.VMEM((experts * slots, tokens), BF16),
            pltpu.VMEM((experts, tokens), F32),
            pltpu.VMEM((tokens, width), BF16),
        ),
        in_specs=[SMEM, VMEM, HBM],
        out_specs=(VMEM,) * 3,
        scratch_shapes=[pltpu.SemaphoreType.DMA],
        compiler_params=room(8),
        name="slots",
    )(place, far(ids), far(residual))
    order = lax.axis_size("sp")
    head = lax.ppermute(tail, "sp", [(i, i + 1) for i in range(order - 1)])
    own_out = lax.all_to_all(packed, "y", 0, 0, tiled=True)
    sent = group + gains.shape[0]
    filtered = pl.pallas_call(
        filter_kernel,
        out_shape=pltpu.VMEM((sent, tokens), BF16),
        in_specs=[VMEM] * 4,
        out_specs=VMEM,
        compiler_params=room(4),
        name="filter",
    )(near(head), near(gated), near(taps), near(gains))
    rows = lax.all_gather(filtered, TP, axis=0, tiled=True)
    other_out = twin(own_out)
    rows = rows.reshape(chips, 2, sent, tokens)
    gates = (expert_gate[0], twin(expert_gate[0]))
    ups = (expert_up[0], twin(expert_up[0]))
    downs = (expert_down[0], twin(expert_down[0]))

    updated, send = pl.pallas_call(
        token_kernel,
        out_shape=(
            pltpu.VMEM((tokens, mine), F32),
            pltpu.VMEM((experts, slots, width), BF16),
        ),
        in_specs=[SMEM] + [VMEM] * 5,
        out_specs=(VMEM,) * 2,
        compiler_params=room(12),
        name="token",
    )(place, near(rows), near(own_out), near(other_out), near(pick), near(res))

    arrived = lax.all_to_all(send, "sp", 0, 0, tiled=True).reshape(1, experts * slots, width)
    full = lax.all_gather(arrived, "y", axis=0, tiled=True)
    parts, part = 2, full.shape[1] // 2
    partial = pl.pallas_call(
        expert_kernel,
        out_shape=pltpu.HBM(full.shape, BF16),
        in_specs=[HBM] + [VMEM] * 2 + [HBM] * 4,
        out_specs=HBM,
        scratch_shapes=[
            pltpu.VMEM((parts, chips, part, width), BF16),
            pltpu.VMEM((2, *ups[0].shape), BF16),
            pltpu.VMEM((2 * downs[0].shape[0], model), BF16),
            pltpu.VMEM((parts, chips, part, width), BF16),
            pltpu.SemaphoreType.DMA((parts,)),
            pltpu.SemaphoreType.DMA((2,)),
            pltpu.SemaphoreType.DMA((2,)),
            pltpu.SemaphoreType.DMA((parts, chips)),
        ],
        compiler_params=room(32),
        name="expert",
    )(far(full), *(near(w) for w in gates), *(far(w) for w in (*ups, *downs)))
    summed = lax.psum_scatter(partial, "y", scatter_dimension=0, tiled=True)
    back = lax.all_to_all(summed.reshape(experts, slots, width), "sp", 0, 0, tiled=True)
    kept, given = pl.pallas_call(
        combine_kernel,
        out_shape=(pltpu.VMEM((tokens, mine), F32), pltpu.VMEM((tokens, mine), F32)),
        in_specs=[SMEM] + [VMEM] * 5,
        out_specs=(VMEM,) * 2,
        compiler_params=room(8),
        name="combine",
    )(place, near(back), near(rank), near(ids), near(weights), near(updated))
    return (kept + twin(given)).astype(BF16)


def solution(mesh):
    grid = Mesh(mesh.devices.reshape(mesh.shape["sp"], 8, 2), ("sp", "y", "c"))
    placed = (
        P("sp", TP),
        P("sp", TP),
        P(None, TP),
        P(TP),
        P(TP, None),
        P("sp", None),
        P("sp", None),
        P("sp", None),
        P("sp", None, TP),
        P("sp", None, TP),
        P("sp", TP, None),
    )

    return jax.shard_map(local, mesh=grid, in_specs=placed, out_specs=P("sp", TP), check_vma=False)
```
